32 devices in a mesh: grp: 2 (over y), ep: 4 (over z), tp: 4 (over x, core).
Axes of the slice: x: 2, y: 2, z: 4, core: 2. Of those that a mesh axis runs over, the one named last changes fastest.
Arguments:
- tokens: bfloat16 [2048, 2048], P(('grp', 'ep'), 'tp'), parts along dimension 0, may hold values from -6 to 6
- norm_gain: float32 [2048], replicated, may hold values from 0.1 to 1.9
- expert_ids: int32 [2048, 2], P(('grp', 'ep')), parts along dimension 0, may hold values from 0 to 3, all different within a row; in each aligned block of 256 rows (0 to 255, 256 to 511, ...) at most 192 rows name the same one
- gate_weights: float32 [2048, 2], P(('grp', 'ep')), parts along dimension 0, may hold values from 0.25 to 1
- w_gate: bfloat16 [4, 2048, 3072], P('ep', None, 'tp'), may hold values from -0.125 to 0.125
- w_up: bfloat16 [4, 2048, 3072], P('ep', None, 'tp'), may hold values from -0.125 to 0.125
- w_down: bfloat16 [4, 3072, 2048], P('ep', 'tp'), may hold values from -0.15625 to 0.15625
Outputs:
- mixed: bfloat16 [2048, 2048], P(('grp', 'ep'), 'tp'), parts along dimension 0
The draws below stay inside these ranges and needn't reach their ends.
There are 2 independent parts, one for each index of `grp`. The reference program is written for one: setup_inputs(seed, part) draws one part's arguments, and reference() takes and returns one part's arrays. A program takes and returns all parts, laid end to end along the dimension named above; an argument that names none is the same for every part. Nothing has to cross between parts.
Inputs may be any that keep to these rules, and one draw needn't show every extreme that they name: `expert_ids`: each token names 2 different experts. Within the 256 rows of one index of ep (aligned blocks) no expert is named more than 192 times, and in some blocks one expert is named exactly 192 times.
All inputs are finite; a program needn't handle non-finite values.
Results may differ from the reference program's by a relative error of at most 0.015.
Values may be sent and summed in bfloat16 or wider, within the bound.
A program may use at most 64 MiB of HBM per device.

```python
import math
import jax
import jax.numpy as jnp
import numpy as np
from jax import lax

D = 2048
FF = 3072
TOP = 2
TOK_DEV = 256
EXPERTS = 4
CAP = 192
TOKENS = 1024
N_EP = 4
N_TP = 4


def with_spikes(result, stream_key, source, target, blocks, factor):
    def block_of(dim):
        return (jnp.arange(result.shape[dim]) // (result.shape[dim] // blocks)).reshape((-1,) + (1,) * (result.ndim - 1 - dim))

    one_side = jax.random.permutation(stream_key, blocks)[block_of(target)]
    other_side = (block_of(target) + blocks // 2) % blocks
    return jnp.where((block_of(source) == one_side) | (block_of(source) == other_side), factor * result, result)


def block_levels(own_key, extent, shards, least, top_value):
    def one(dim, parts):
        steps = jax.random.uniform(jax.random.fold_in(jax.random.fold_in(own_key, 6), dim), (parts,), jnp.float32, least / len(shards), top_value / len(shards))
        return jnp.repeat(jnp.exp(steps), extent[dim] // parts).reshape((-1,) + (1,) * (len(extent) - dim - 1))

    level = one(*shards[0])
    for cut in shards[1:]:
        level = level * one(*cut)
    return level


def deal_out(key, own, number, rows, amount, top, reach, slope):
    ranking = jax.random.permutation(key, amount)
    packed, ordinary = shares(amount, rows * top, reach, slope, True), shares(amount, rows * top, reach, slope, False)
    places = jnp.arange(amount)

    def named(lengths, turn):
        used = int((lengths > 0).sum())
        fixed = max(1, used // 4)
        passed = fixed + (places - fixed + turn * (used - fixed)) % max(1, amount - fixed)
        return jnp.zeros((amount,), jnp.int32).at[ranking[jnp.where(places < fixed, places, passed)]].set(jnp.asarray(lengths, jnp.int32))

    lengths = jnp.where(number % 4 == 0, named(packed, number // 4), named(ordinary, number - number // 4 - 1))
    mixed = jax.random.permutation(jax.random.fold_in(own, 3), amount)
    donor, receiver = mixed[0:amount // 2 * 2:2], mixed[1:amount // 2 * 2:2]
    slack = jnp.minimum(lengths[donor] - 1, reach - lengths[receiver]) // 2
    slack = jnp.where((donor == ranking[0]) | (receiver == ranking[0]) | (lengths[receiver] == 0), 0, jnp.maximum(slack, 0))
    passed = jax.random.randint(jax.random.fold_in(own, 4), (amount // 2,), 0, 1 << 20) % (slack + 1)
    lengths = lengths.at[donor].add(-passed).at[receiver].add(passed)
    members = jnp.searchsorted(jnp.cumsum(lengths), jnp.arange(rows * top), side="right").astype(jnp.int32)
    listing = members.reshape(top, rows).T
    listing = listing[jax.random.permutation(jax.random.fold_in(own, 1), rows)]
    turn = jax.random.randint(jax.random.fold_in(own, 2), (rows, 1), 0, top)
    return jnp.take_along_axis(listing, (jnp.arange(top)[None, :] + turn) % top, axis=1)


def shares(number_of, total, bound, skew, full):
    portions = [(1 << 20) // math.isqrt(rank ** skew) + 1 for rank in range(1, number_of + 1)]
    largest = bound if full else min(bound, max(-(-total // number_of), total * portions[0] // sum(portions)))
    least = 1 if total - largest >= number_of - 1 else 0
    given, spare = [largest] + [least] * (number_of - 1), total - largest - least * (number_of - 1)
    while spare > 0:
        free = [i for i in range(1, number_of) if given[i] < largest] or [i for i in range(1, number_of) if given[i] < bound]
        pool, budget = sum([portions[i] for i in free]), spare
        for i in free:
            extra = min(bound - given[i], max(1, budget * portions[i] // pool), spare)
            given[i] = given[i] + extra
            spare = spare - extra
    return np.array(given)


def gaussian(key, dims, spread, bound, split=(), kind=jnp.bfloat16):
    array = jax.random.normal(key, dims, jnp.float32) * spread
    if len(split) > 0:
        array = block_levels(key, dims, split, -0.22, 0.18) * array
    return jnp.clip(array, min=-bound, max=bound).astype(kind)


def heavy_noise(key, shape, spread, most, shards, heavy, kind=jnp.bfloat16):
    values = spread * jax.random.normal(key, shape, jnp.float32)
    if shards:
        values = values * block_levels(key, shape, shards, -0.22, 0.18)
    return jnp.clip(with_spikes(values, jax.random.fold_in(key, 3), *heavy), -most, most).astype(kind)


def setup_inputs(seed: int = 0, part: int = 0) -> dict:
    seeds = jax.random.split(jax.random.key(seed), 8)
    own_keys = jax.random.split(jax.random.fold_in(seeds[7], part), 8)
    tokens = gaussian(own_keys[0], (TOKENS, D), 1.0, 6.0, ((0, 4), (1, 4)))
    norm_gain = jnp.clip(1.0 + 0.18 * jax.random.normal(seeds[1], (D,), jnp.float32), 0.1, 1.9)
    expert_ids_keys = jax.random.split(jax.random.fold_in(own_keys[2], 1), TOKENS // TOK_DEV)
    expert_ids_turns = jax.random.permutation(jax.random.fold_in(own_keys[2], 3), TOKENS // TOK_DEV)
    expert_ids = jax.vmap(lambda own, number: deal_out(jax.random.fold_in(own_keys[2], 2), own, number, TOK_DEV, EXPERTS, TOP, CAP, 2))(expert_ids_keys, expert_ids_turns).reshape((TOKENS, TOP))
    gate_weights = jnp.clip(0.25 + 0.75 * jax.random.uniform(own_keys[3], (TOKENS, TOP), jnp.float32) ** block_levels(own_keys[3], (TOKENS, TOP), ((0, 4),), -0.2, 0.2), 0.25, 1.0)
    w_gate = gaussian(seeds[4], (EXPERTS, D, FF), D ** -0.5, 0.125, ((0, 4), (2, 4)))
    w_up = gaussian(seeds[5], (EXPERTS, D, FF), D ** -0.5, 0.125, ((0, 4), (2, 4)))
    w_down = heavy_noise(seeds[6], (EXPERTS, FF, D), FF ** -0.5, 0.15625, ((0, 4), (1, 4)), (1, 2, 4, 2.0))
    return dict(tokens=tokens, norm_gain=norm_gain, expert_ids=expert_ids, gate_weights=gate_weights, w_gate=w_gate, w_up=w_up, w_down=w_down)


epsilon = 1e-06

def reference(tokens, norm_gain, expert_ids, gate_weights, w_gate, w_up, w_down):
    tok_values = tokens.astype(jnp.float32)
    mean_square = lax.optimization_barrier(jnp.mean(tok_values * tok_values, axis=1, keepdims=True))
    normed = (tok_values * lax.rsqrt(mean_square + epsilon) * norm_gain.astype(jnp.float32)).astype(jnp.bfloat16)
    assign_count = TOK_DEV * TOP
    block_ids = expert_ids.reshape(N_EP, assign_count)
    onehot = (block_ids[:, :, None] == jnp.arange(EXPERTS, dtype=jnp.int32)[None, None, :]).astype(jnp.int32)
    earlier = jnp.cumsum(onehot, axis=1) - onehot
    slot_index = lax.optimization_barrier(jnp.sum(earlier * onehot, axis=2)).astype(jnp.int32)
    block_index = jnp.arange(N_EP, dtype=jnp.int32)[:, None]
    dest_index = ((block_ids * N_EP + block_index) * CAP + slot_index).astype(jnp.int32)
    owner_index = (block_index * TOK_DEV + jnp.arange(assign_count, dtype=jnp.int32)[None, :] // TOP).astype(jnp.int32)
    slot_token = jnp.full((EXPERTS * N_EP * CAP,), TOKENS, jnp.int32)
    slot_token = slot_token.at[dest_index.reshape(-1)].set(owner_index.reshape(-1))
    slot_token = slot_token.reshape(EXPERTS, N_EP * CAP)

    def run_expert(inputs):
        token_list, gate_matrix, up_matrix, down_matrix = inputs
        tok_rows = jnp.take(normed, token_list, axis=0, mode='fill', fill_value=0)
        gate_part = jnp.dot(tok_rows, gate_matrix, preferred_element_type=jnp.float32)
        up_part = jnp.dot(tok_rows, up_matrix, preferred_element_type=jnp.float32)
        hidden = (jax.nn.silu(gate_part) * up_part).astype(jnp.bfloat16)
        hidden_blocks = hidden.reshape(-1, N_TP, FF // N_TP).astype(jnp.float32)
        down_blocks = down_matrix.reshape(N_TP, FF // N_TP, D).astype(jnp.float32)
        partial_value = jnp.einsum('mtf,tfd->tmd', hidden_blocks, down_blocks).astype(jnp.bfloat16)
        partial_value = lax.optimization_barrier(partial_value)
        return lax.optimization_barrier(jnp.sum(partial_value.astype(jnp.float32), axis=0)).astype(jnp.bfloat16)
    expert_out = lax.map(run_expert, (slot_token, w_gate, w_up, w_down))
    picked = expert_out.reshape(-1, D)[dest_index.reshape(-1)].astype(jnp.float32)
    weighted = picked * gate_weights.reshape(-1)[:, None].astype(jnp.float32)
    return lax.optimization_barrier(jnp.sum(weighted.reshape(TOKENS, TOP, D), axis=1)).astype(jnp.bfloat16)
```

```python
import functools

import jax
import jax.numpy as jnp
from jax import lax
from jax.experimental import pallas as pl
from jax.experimental.pallas import tpu as pltpu
from jax.sharding import PartitionSpec as P

epsilon = 1e-06
AHEAD = 2
LAG = 1
MESH = pl.DeviceIdType.MESH


def nearest_first(count):
    table = []
    for e in range(count):
        mirrored = 1 if 2 * e < count else -1
        table.append(sorted(range(count), key=lambda s: (abs(s - e), mirrored * s)))
    return table


def mirrored(units, count):
    return [(count - 1 - s, h) for s, h in units]


def unit_order(n_ep, cuts):
    if (n_ep, cuts) == (4, 2):
        outer = [(0, 0), (1, 0), (1, 1), (2, 0), (3, 1), (3, 0), (2, 1), (0, 1)]
        inner = [(1, 0), (3, 0), (0, 1), (2, 0), (3, 1), (2, 1), (0, 0), (1, 1)]
        both = [outer, inner, mirrored(inner, 4), mirrored(outer, 4)]
    else:
        both = [
            [(s, h) for s in row for h in range(cuts)] for row in nearest_first(n_ep)
        ]
    return [[s * cuts + h for s, h in row] for row in both]


def send_order(n_ep, cuts):
    if (n_ep, cuts) == (4, 2):
        outer = [(2, 0), (1, 1), (2, 1), (1, 0), (3, 1), (3, 0)]
        inner = [(2, 0), (0, 0), (3, 0), (0, 1), (3, 1), (2, 1)]
        both = [outer, inner, mirrored(inner, 4), mirrored(outer, 4)]
    else:
        both = [
            [(s, h) for s in row[1:] for h in range(cuts)] for row in nearest_first(n_ep)
        ]
    return [[s * cuts + h for s, h in row] for row in both]


def pick_row(table, row):
    picked = []
    for column in range(len(table[0])):
        value = jnp.int32(table[0][column])
        for r in range(1, len(table)):
            value = jnp.where(row == r, table[r][column], value)
        picked.append(value)
    return picked


def entry_of(entries, index):
    value = entries[0]
    for c in range(1, len(entries)):
        value = jnp.where(index == c, entries[c], value)
    return value


def layer_kernel(
    n_ep,
    cap,
    cuts,
    tok_ref,
    ids_ref,
    gate_ref,
    gain_ref,
    wg_ref,
    wu_ref,
    wd_ref,
    out_ref,
    wg,
    wu,
    wd,
    packed,
    rows,
    normed,
    hidden,
    own,
    to_core,
    from_core,
    to_chip,
    from_chip,
    result,
    back,
    w_sem,
    z_send,
    z_recv,
    x_send,
    x_recv,
    d_send,
    d_recv,
    e_send,
    e_recv,
    pc_send,
    pc_recv,
    px_send,
    px_recv,
    r_send,
    r_recv,
):
    tok_count, col_count = tok_ref.shape
    top_count = ids_ref.shape[0]
    n_tp = rows.shape[1]
    width = n_tp * col_count
    ep = lax.axis_index("ep")
    tp = lax.axis_index("tp")
    core = tp % 2
    sibling = tp + 1 - 2 * core
    across = (tp + 2) % n_tp
    side = tp // 2
    table = nearest_first(n_ep)
    order = pick_row(table, ep)
    units = pick_row(unit_order(n_ep, cuts), ep)
    sends = pick_row(send_order(n_ep, cuts), ep)

    weights = [
        pltpu.make_async_copy(wg_ref.at[0], wg, w_sem.at[0]),
        pltpu.make_async_copy(wu_ref.at[0], wu, w_sem.at[1]),
    ]
    piece_of = [
        (1 - side) * 2 + 1 - core,
        side * 2 + 1 - core,
        (1 - side) * 2 + core,
        side * 2 + core,
    ]
    for j, piece in enumerate(piece_of):
        cols = pl.ds(pl.multiple_of(piece * col_count, col_count), col_count)
        weights.append(
            pltpu.make_async_copy(wd_ref.at[0, :, cols], wd.at[j], w_sem.at[2 + j])
        )
    for copy in weights:
        copy.start()

    barrier = pltpu.get_barrier_semaphore()
    for step in range(1, n_ep):
        pl.semaphore_signal(
            barrier, inc=1, device_id={"ep": (ep + step) % n_ep}, device_id_type=MESH
        )
    for peer in (sibling, across):
        pl.semaphore_signal(barrier, inc=1, device_id={"tp": peer}, device_id_type=MESH)

    lane = lax.broadcasted_iota(jnp.int32, (tok_count, 128), 1)
    lane_expert = jnp.full((tok_count, 128), -1, jnp.int32)
    for i in range(n_ep):
        lane_expert = jnp.where(lane == i, order[i], lane_expert)
    ids = ids_ref[...].astype(jnp.float32).T
    gates = gate_ref[...].T
    lane_expert = lane_expert.astype(jnp.float32)
    named = jnp.zeros((tok_count, 128), jnp.float32)
    weight = jnp.zeros((tok_count, 128), jnp.float32)
    for k in range(top_count):
        hit = ids[:, k : k + 1] == lane_expert
        named = named + jnp.where(hit, 1.0, 0.0)
        weight = weight + jnp.where(hit, gates[:, k : k + 1], 0.0)
    before = jnp.where(
        lax.broadcasted_iota(jnp.int32, (tok_count, tok_count), 1)
        < lax.broadcasted_iota(jnp.int32, (tok_count, tok_count), 0),
        1.0,
        0.0,
    ).astype(jnp.bfloat16)
    place = jnp.dot(before, named.astype(jnp.bfloat16), preferred_element_type=jnp.float32)
    place = jnp.where(named > 0.0, place, -1.0)
    place_t = place.T
    slot_rows = lax.broadcasted_iota(jnp.int32, (cap, tok_count), 0).astype(jnp.float32)

    def pack(i):
        pick = jnp.where(slot_rows == place_t[i : i + 1, :], 1.0, 0.0).astype(jnp.bfloat16)
        return jnp.dot(pick, tok_ref[...], preferred_element_type=jnp.float32).astype(
            jnp.bfloat16
        )

    def z_copy(here, there, h):
        return pltpu.make_async_remote_copy(
            src_ref=packed.at[there * cuts + h],
            dst_ref=rows.at[here * cuts + h, tp],
            send_sem=z_send.at[there * cuts + h],
            recv_sem=z_recv.at[here * cuts + h],
            device_id={"ep": there},
            device_id_type=MESH,
        )

    def x_copy(i):
        return pltpu.make_async_remote_copy(
            src_ref=rows.at[i, tp],
            dst_ref=rows.at[i, tp],
            send_sem=x_send.at[i],
            recv_sem=x_recv.at[i],
            device_id={"tp": across},
            device_id_type=MESH,
        )

    def d_copy(i):
        return pltpu.make_async_remote_copy(
            src_ref=rows.at[i, tp],
            dst_ref=rows.at[i, tp],
            send_sem=d_send.at[i],
            recv_sem=d_recv.at[i],
            device_id={"tp": sibling},
            device_id_type=MESH,
        )

    def e_copy(i):
        return pltpu.make_async_remote_copy(
            src_ref=rows.at[i, across],
            dst_ref=rows.at[i, across],
            send_sem=e_send.at[i],
            recv_sem=e_recv.at[i],
            device_id={"tp": sibling},
            device_id_type=MESH,
        )

    def pc_copy(i, j):
        return pltpu.make_async_remote_copy(
            src_ref=to_core.at[i, j],
            dst_ref=from_core.at[i, j],
            send_sem=pc_send.at[i, j],
            recv_sem=pc_recv.at[i, j],
            device_id={"tp": sibling},
            device_id_type=MESH,
        )

    def px_copy(i):
        return pltpu.make_async_remote_copy(
            src_ref=to_chip.at[i],
            dst_ref=from_chip.at[i],
            send_sem=px_send.at[i],
            recv_sem=px_recv.at[i],
            device_id={"tp": across},
            device_id_type=MESH,
        )

    def r_copy(here, there, h):
        return pltpu.make_async_remote_copy(
            src_ref=result.at[there * cuts + h],
            dst_ref=back.at[here * cuts + h],
            send_sem=r_send.at[there * cuts + h],
            recv_sem=r_recv.at[here * cuts + h],
            device_id={"ep": there},
            device_id_type=MESH,
        )

    piece_rows = cap // cuts
    stages = n_ep * cuts
    for i in range(1, n_ep):
        values = pack(i)
        for h in range(cuts):
            packed[order[i] * cuts + h] = values[h * piece_rows : (h + 1) * piece_rows]
    values = pack(0)
    for h in range(cuts):
        rows[ep * cuts + h, tp] = values[h * piece_rows : (h + 1) * piece_rows]

    def unit_of(i):
        return units[i] if isinstance(i, int) else entry_of(units, i)

    def forward(i):
        s = unit_of(i)

        @pl.when(s // cuts != ep)
        def _():
            z_copy(s // cuts, s // cuts, s % cuts).wait_recv()

        x_copy(s).start()
        d_copy(s).start()

    pl.semaphore_wait(barrier, n_ep + 1)
    for unit in sends:
        z_copy(ep, unit // cuts, unit % cuts).start()
    forward(0)
    for copy in weights:
        copy.wait()

    def finish(i):
        s = unit_of(i)
        pc_copy(s, 1).wait_recv()
        total = own[i % (LAG + 1)] + from_core[s, 1].astype(jnp.float32)
        px_copy(s).wait_recv()
        total = total + from_chip[s].astype(jnp.float32)
        result[s] = total.astype(jnp.bfloat16)

        @pl.when(s // cuts != ep)
        def _():
            r_copy(ep, s // cuts, s % cuts).start()

    for i in range(1, AHEAD):
        forward(i)
    x_copy(unit_of(0)).wait_recv()
    e_copy(unit_of(0)).start()

    def stage(i, carry):
        s = unit_of(i)
        d_copy(s).wait_recv()
        e_copy(s).wait_recv()
        square_sum = jnp.zeros((piece_rows, 1), jnp.float32)
        for k in range(n_tp):
            part = rows[s, k].astype(jnp.float32)
            square_sum = square_sum + jnp.sum(part * part, axis=1, keepdims=True)
        factor = lax.rsqrt(square_sum / width + epsilon)
        for k in range(n_tp):
            cols = slice(k * col_count, (k + 1) * col_count)
            part = rows[s, k].astype(jnp.float32)
            normed[:, cols] = (part * factor * gain_ref[:, cols]).astype(jnp.bfloat16)
        gate_part = jnp.dot(normed[...], wg[...], preferred_element_type=jnp.float32)
        up_part = jnp.dot(normed[...], wu[...], preferred_element_type=jnp.float32)
        hidden[...] = (gate_part / (1.0 + jnp.exp(-gate_part)) * up_part).astype(jnp.bfloat16)
        @pl.when(i + AHEAD < stages)
        def _():
            forward(i + AHEAD)

        @pl.when(i + 1 < stages)
        def _():
            after = unit_of(i + 1)
            x_copy(after).wait_recv()
            e_copy(after).start()

        for j in range(2):
            to_core[s, j] = jnp.dot(
                hidden[...], wd[j], preferred_element_type=jnp.float32
            ).astype(jnp.bfloat16)
            pc_copy(s, j).start()
        part = jnp.dot(hidden[...], wd[2], preferred_element_type=jnp.float32)
        own[i % (LAG + 1)] = jnp.dot(hidden[...], wd[3], preferred_element_type=jnp.float32)
        pc_copy(s, 0).wait_recv()
        to_chip[s] = (part + from_core[s, 0].astype(jnp.float32)).astype(jnp.bfloat16)
        px_copy(s).start()

        @pl.when(i >= LAG)
        def _():
            finish(i - LAG)

        return carry

    lax.fori_loop(0, stages, stage, 0)
    for i in range(stages - LAG, stages):
        finish(i)

    slot_lanes = lax.broadcasted_iota(jnp.int32, (tok_count, piece_rows), 1).astype(
        jnp.float32
    )
    mixed = jnp.zeros((tok_count, col_count), jnp.float32)
    for i in range(n_ep):
        taken = jnp.zeros((tok_count, col_count), jnp.float32)
        for h in range(cuts):
            pick = jnp.where(slot_lanes + h * piece_rows == place[:, i : i + 1], 1.0, 0.0)
            unit = order[i] * cuts + h
            if i == 0:
                values = result[unit]
            else:
                r_copy(order[i], order[i], h).wait_recv()
                values = back[unit]
            taken = taken + jnp.dot(
                pick.astype(jnp.bfloat16), values, preferred_element_type=jnp.float32
            )
        mixed = mixed + weight[:, i : i + 1] * taken
    out_ref[...] = mixed.astype(jnp.bfloat16)

    for i in range(1, n_ep):
        for h in range(cuts):
            z_copy(ep, order[i], h).wait_send()
            r_copy(ep, order[i], h).wait_send()
    for i in range(stages):
        x_copy(i).wait_send()
        d_copy(i).wait_send()
        e_copy(i).wait_send()
        pc_copy(i, 0).wait_send()
        pc_copy(i, 1).wait_send()
        px_copy(i).wait_send()


def fused(tokens, norm_gain, expert_ids, gate_weights, w_gate, w_up, w_down):
    tok_count, col_count = tokens.shape
    top_count = expert_ids.shape[1]
    n_ep = lax.axis_size("ep")
    n_tp = lax.axis_size("tp")
    cap = 3 * tok_count * top_count // (2 * n_ep)
    cuts = 2 if cap % 32 == 0 else 1
    stages, piece_rows = n_ep * cuts, cap // cuts
    width = norm_gain.shape[0]
    units = w_gate.shape[2]
    bf16 = jnp.bfloat16
    vmem = pl.BlockSpec(memory_space=pltpu.VMEM)
    anywhere = pl.BlockSpec(memory_space=pl.ANY)
    sems = pltpu.SemaphoreType.DMA
    return pl.pallas_call(
        functools.partial(layer_kernel, n_ep, cap, cuts),
        out_shape=jax.ShapeDtypeStruct((tok_count, col_count), bf16),
        in_specs=[vmem] * 4 + [anywhere] * 3,
        out_specs=vmem,
        scratch_shapes=[
            pltpu.VMEM((width, units), bf16),
            pltpu.VMEM((width, units), bf16),
            pltpu.VMEM((n_tp, units, col_count), bf16),
            pltpu.VMEM((stages, piece_rows, col_count), bf16),
            pltpu.VMEM((stages, n_tp, piece_rows, col_count), bf16),
            pltpu.VMEM((piece_rows, width), bf16),
            pltpu.VMEM((piece_rows, units), bf16),
            pltpu.VMEM((LAG + 1, piece_rows, col_count), jnp.float32),
            pltpu.VMEM((stages, 2, piece_rows, col_count), bf16),
            pltpu.VMEM((stages, 2, piece_rows, col_count), bf16),
        ]
        + [pltpu.VMEM((stages, piece_rows, col_count), bf16)] * 4
        + [sems((2 + n_tp,))]
        + [sems((stages,))] * 8
        + [sems((stages, 2))] * 2
        + [sems((stages,))] * 4,
        compiler_params=pltpu.CompilerParams(
            collective_id=0, has_side_effects=True, vmem_limit_bytes=56 * 2**20
        ),
    )(
        tokens,
        expert_ids.T,
        gate_weights.T,
        norm_gain.reshape(1, width),
        w_gate,
        w_up,
        w_down,
    )


def on_device(tokens, norm_gain, expert_ids, gate_weights, w_gate, w_up, w_down):
    tok_count = tokens.shape[0]
    top_count = expert_ids.shape[1]
    expert_count = lax.axis_size("ep")
    capacity = 3 * tok_count * top_count // (2 * expert_count)
    model_width = norm_gain.shape[0]
    flat_ids = expert_ids.reshape(-1)
    onehot = (flat_ids[:, None] == jnp.arange(expert_count, dtype=jnp.int32)[None, :]).astype(
        jnp.int32
    )
    earlier = jnp.cumsum(onehot, axis=0) - onehot
    slot_index = jnp.sum(earlier * onehot, axis=1)
    dest_index = flat_ids * capacity + slot_index
    owner_index = jnp.arange(tok_count * top_count, dtype=jnp.int32) // top_count
    slot_token = (
        jnp.full((expert_count * capacity,), tok_count, jnp.int32).at[dest_index].set(owner_index)
    )
    tok_values = tokens.astype(jnp.float32)
    square_sum = lax.psum(jnp.sum(tok_values * tok_values, axis=1, keepdims=True), "tp")
    col_count = tokens.shape[1]
    gain_part = lax.dynamic_slice_in_dim(norm_gain, lax.axis_index("tp") * col_count, col_count)
    normed = (tok_values * lax.rsqrt(square_sum / model_width + epsilon) * gain_part).astype(
        jnp.bfloat16
    )
    buffer = jnp.take(normed, slot_token, axis=0, mode="fill", fill_value=0).reshape(
        expert_count, capacity, -1
    )
    received = lax.all_to_all(buffer, "ep", split_axis=0, concat_axis=0, tiled=True)
    source_count, item_count, col_count = received.shape
    tok_rows = received.reshape(-1, col_count)
    col_piece = lax.all_gather(tok_rows, "tp", axis=1, tiled=True)
    gate_rows = w_gate[0]
    up_rows = w_up[0]
    gate_part = jnp.dot(col_piece, gate_rows, preferred_element_type=jnp.float32)
    up_part = jnp.dot(col_piece, up_rows, preferred_element_type=jnp.float32)
    hidden = (jax.nn.silu(gate_part) * up_part).astype(jnp.bfloat16)
    partial_value = jnp.dot(hidden, w_down[0], preferred_element_type=jnp.float32)
    partial_value = partial_value.reshape(source_count, item_count, -1)
    summed = lax.psum_scatter(
        partial_value.astype(jnp.bfloat16), "tp", scatter_dimension=2, tiled=True
    )
    came_back = lax.all_to_all(summed, "ep", split_axis=0, concat_axis=0, tiled=True)
    picked = came_back.reshape(expert_count * capacity, -1)[dest_index].astype(jnp.float32)
    weighted = picked * gate_weights.reshape(-1)[:, None]
    return jnp.sum(weighted.reshape(tok_count, top_count, -1), axis=1).astype(jnp.bfloat16)


def solution(mesh):
    return jax.shard_map(
        fused if mesh.shape["tp"] == 4 else on_device,
        mesh=mesh,
        in_specs=(
            P(("grp", "ep"), "tp"),
            P(),
            P(("grp", "ep"), None),
            P(("grp", "ep"), None),
            P("ep", None, "tp"),
            P("ep", None, "tp"),
            P("ep", "tp", None),
        ),
        out_specs=P(("grp", "ep"), "tp"),
        check_vma=False,
    )
```

```python
import functools

import jax
import jax.numpy as jnp
from jax import lax
from jax.experimental import pallas as pl
from jax.experimental.pallas import tpu as pltpu
from jax.sharding import PartitionSpec as P

epsilon = 1e-06
AHEAD = 2
LAG = 1
MESH = pl.DeviceIdType.MESH


def nearest_first(count):
    table = []
    for e in range(count):
        mirrored = 1 if 2 * e < count else -1
        table.append(sorted(range(count), key=lambda s: (abs(s - e), mirrored * s)))
    return table


def mirrored(units, count):
    return [(count - 1 - s, h) for s, h in units]


def unit_order(n_ep, cuts):
    if (n_ep, cuts) == (4, 2):
        outer = [(0, 1), (1, 0), (2, 1), (3, 0), (3, 1), (2, 0), (1, 1), (0, 0)]
        inner = [(1, 1), (3, 0), (0, 1), (2, 0), (3, 1), (0, 0), (2, 1), (1, 0)]
        both = [outer, inner, mirrored(inner, 4), mirrored(outer, 4)]
    else:
        both = [
            [(row[0], h) for h in range(cuts - 1)]
            + [(s, h) for s in row[1:] for h in range(cuts)]
            + [(row[0], cuts - 1)]
            for row in nearest_first(n_ep)
        ]
    return [[s * cuts + h for s, h in row] for row in both]


def send_order(n_ep, cuts):
    if (n_ep, cuts) == (4, 2):
        outer = [(2, 0), (1, 1), (1, 0), (3, 0), (2, 1), (3, 1)]
        inner = [(0, 0), (3, 1), (2, 0), (2, 1), (3, 0), (0, 1)]
        both = [outer, inner, mirrored(inner, 4), mirrored(outer, 4)]
    else:
        both = [
            [(s, h) for s in row[1:] for h in range(cuts)] for row in nearest_first(n_ep)
        ]
    return [[s * cuts + h for s, h in row] for row in both]


def pick_row(table, row):
    picked = []
    for column in range(len(table[0])):
        value = jnp.int32(table[0][column])
        for r in range(1, len(table)):
            value = jnp.where(row == r, table[r][column], value)
        picked.append(value)
    return picked


def entry_of(entries, index):
    value = entries[0]
    for c in range(1, len(entries)):
        value = jnp.where(index == c, entries[c], value)
    return value


def layer_kernel(
    n_ep,
    cap,
    cuts,
    tok_hbm,
    ids_hbm,
    gate_hbm,
    gain_hbm,
    wg_ref,
    wu_ref,
    wd_ref,
    out_ref,
    tok_ref,
    ids_ref,
    gate_ref,
    gain_ref,
    acc,
    wg,
    wu,
    wd,
    packed,
    rows,
    hidden,
    own,
    to_core,
    from_core,
    to_chip,
    from_chip,
    result,
    back,
    w_sem,
    i_sem,
    z_send,
    z_recv,
    x_send,
    x_recv,
    d_send,
    d_recv,
    e_send,
    e_recv,
    pc_send,
    pc_recv,
    px_send,
    px_recv,
    r_send,
    r_recv,
):
    tok_count, col_count = tok_ref.shape
    top_count = ids_ref.shape[0]
    n_tp = rows.shape[1]
    units = wg.shape[1]
    width = n_tp * col_count
    ep = lax.axis_index("ep")
    tp = lax.axis_index("tp")
    core = tp % 2
    sibling = tp + 1 - 2 * core
    across = (tp + 2) % n_tp
    side = tp // 2
    barrier = pltpu.get_barrier_semaphore()
    for step in range(1, n_ep):
        pl.semaphore_signal(
            barrier, inc=1, device_id={"ep": (ep + step) % n_ep}, device_id_type=MESH
        )
    for peer in (sibling, across):
        pl.semaphore_signal(barrier, inc=1, device_id={"tp": peer}, device_id_type=MESH)

    inputs = [
        pltpu.make_async_copy(source, target, i_sem.at[n])
        for n, (source, target) in enumerate(
            [
                (ids_hbm, ids_ref),
                (gate_hbm, gate_ref),
                (tok_hbm, tok_ref),
                (gain_hbm, gain_ref),
            ]
        )
    ]
    for copy in inputs:
        copy.start()

    table = nearest_first(n_ep)
    order = pick_row(table, ep)
    turns = pick_row(unit_order(n_ep, cuts), ep)
    sends = pick_row(send_order(n_ep, cuts), ep)

    weights = [
        pltpu.make_async_copy(wg_ref.at[0], wg, w_sem.at[0]),
        pltpu.make_async_copy(wu_ref.at[0], wu, w_sem.at[1]),
    ]
    piece_of = [
        (1 - side) * 2 + 1 - core,
        side * 2 + 1 - core,
        (1 - side) * 2 + core,
        side * 2 + core,
    ]
    for j, piece in enumerate(piece_of):
        cols = pl.ds(pl.multiple_of(piece * col_count, col_count), col_count)
        weights.append(
            pltpu.make_async_copy(wd_ref.at[0, :, cols], wd.at[j], w_sem.at[2 + j])
        )
    inputs[0].wait()
    inputs[1].wait()
    lane = lax.broadcasted_iota(jnp.int32, (tok_count, 128), 1)
    lane_expert = jnp.full((tok_count, 128), -1, jnp.int32)
    for i in range(n_ep):
        lane_expert = jnp.where(lane == i, order[i], lane_expert)
    ids = ids_ref[...].astype(jnp.float32).T
    gates = gate_ref[...].T
    lane_expert = lane_expert.astype(jnp.float32)
    named = jnp.zeros((tok_count, 128), jnp.float32)
    weight = jnp.zeros((tok_count, 128), jnp.float32)
    for k in range(top_count):
        hit = ids[:, k : k + 1] == lane_expert
        named = named + jnp.where(hit, 1.0, 0.0)
        weight = weight + jnp.where(hit, gates[:, k : k + 1], 0.0)
    before = jnp.where(
        lax.broadcasted_iota(jnp.int32, (tok_count, tok_count), 1)
        < lax.broadcasted_iota(jnp.int32, (tok_count, tok_count), 0),
        1.0,
        0.0,
    ).astype(jnp.bfloat16)
    place = jnp.dot(before, named.astype(jnp.bfloat16), preferred_element_type=jnp.float32)
    place = jnp.where(named > 0.0, place, -1.0)
    place_t = place.T
    slot_rows = lax.broadcasted_iota(jnp.int32, (cap, tok_count), 0).astype(jnp.float32)

    def pack(i):
        pick = jnp.where(slot_rows == place_t[i : i + 1, :], 1.0, 0.0).astype(jnp.bfloat16)
        return jnp.dot(pick, tok_ref[...], preferred_element_type=jnp.float32).astype(
            jnp.bfloat16
        )

    def z_copy(here, there, h):
        return pltpu.make_async_remote_copy(
            src_ref=packed.at[there * cuts + h],
            dst_ref=rows.at[here * cuts + h, tp],
            send_sem=z_send,
            recv_sem=z_recv.at[here * cuts + h],
            device_id={"ep": there},
            device_id_type=MESH,
        )

    def x_copy(i):
        return pltpu.make_async_remote_copy(
            src_ref=rows.at[i, tp],
            dst_ref=rows.at[i, tp],
            send_sem=x_send,
            recv_sem=x_recv.at[i],
            device_id={"tp": across},
            device_id_type=MESH,
        )

    def d_copy(i):
        return pltpu.make_async_remote_copy(
            src_ref=rows.at[i, tp],
            dst_ref=rows.at[i, tp],
            send_sem=d_send,
            recv_sem=d_recv.at[i],
            device_id={"tp": sibling},
            device_id_type=MESH,
        )

    def e_copy(i):
        return pltpu.make_async_remote_copy(
            src_ref=rows.at[i, across],
            dst_ref=rows.at[i, across],
            send_sem=e_send,
            recv_sem=e_recv.at[i],
            device_id={"tp": sibling},
            device_id_type=MESH,
        )

    def pc_copy(i, j):
        return pltpu.make_async_remote_copy(
            src_ref=to_core.at[i, j],
            dst_ref=from_core.at[i, j],
            send_sem=pc_send,
            recv_sem=pc_recv.at[i, j],
            device_id={"tp": sibling},
            device_id_type=MESH,
        )

    def px_copy(i):
        return pltpu.make_async_remote_copy(
            src_ref=to_chip.at[i],
            dst_ref=from_chip.at[i],
            send_sem=px_send,
            recv_sem=px_recv.at[i],
            device_id={"tp": across},
            device_id_type=MESH,
        )

    def r_copy(here, there, h):
        return pltpu.make_async_remote_copy(
            src_ref=result.at[there * cuts + h],
            dst_ref=back.at[here * cuts + h],
            send_sem=r_send,
            recv_sem=r_recv.at[here * cuts + h],
            device_id={"ep": there},
            device_id_type=MESH,
        )

    piece_rows = cap // cuts
    stages = n_ep * cuts
    inputs[2].wait()
    for copy in weights:
        copy.start()
    for i in range(1, n_ep):
        values = pack(i)
        for h in range(cuts):
            packed[order[i] * cuts + h] = values[h * piece_rows : (h + 1) * piece_rows]
    values = pack(0)
    for h in range(cuts):
        rows[ep * cuts + h, tp] = values[h * piece_rows : (h + 1) * piece_rows]

    def unit_of(i):
        return turns[i] if isinstance(i, int) else entry_of(turns, i)

    def spread(s):
        x_copy(s).start()
        d_copy(s).start()

    def forward(i):
        s = unit_of(i)

        @pl.when(s // cuts != ep)
        def _():
            z_copy(s // cuts, s // cuts, s % cuts).wait_recv()
            spread(s)

    pl.semaphore_wait(barrier, n_ep + 1)
    for unit in sends:
        z_copy(ep, unit // cuts, unit % cuts).start()
    for h in range(cuts):
        spread(ep * cuts + h)
    inputs[3].wait()
    for copy in weights:
        copy.wait()

    def scale(i, carry):
        block = pl.ds(pl.multiple_of(i * 128, 128), 128)
        gain = jnp.broadcast_to(gain_ref[:, block], (128, 128)).T
        for matrix in (wg, wu):
            for c in range(units // 128):
                cols = slice(c * 128, (c + 1) * 128)
                matrix[block, cols] = (matrix[block, cols].astype(jnp.float32) * gain).astype(
                    jnp.bfloat16
                )
        return carry

    lax.fori_loop(0, width // 128, scale, 0)

    def finish(i):
        s = unit_of(i)
        pc_copy(s, 1).wait_recv()
        total = own[i % (LAG + 1)] + from_core[s, 1].astype(jnp.float32)
        px_copy(s).wait_recv()
        total = total + from_chip[s].astype(jnp.float32)
        result[s] = total.astype(jnp.bfloat16)

        @pl.when(s // cuts != ep)
        def _():
            r_copy(ep, s // cuts, s % cuts).start()

    for i in range(1, AHEAD):
        forward(i)
    x_copy(unit_of(0)).wait_recv()
    e_copy(unit_of(0)).start()

    def stage(i, carry):
        s = unit_of(i)
        d_copy(s).wait_recv()
        e_copy(s).wait_recv()
        square_sum = jnp.zeros((piece_rows, 1), jnp.float32)
        for k in range(n_tp):
            part = rows[s, k].astype(jnp.float32)
            square_sum = square_sum + jnp.sum(part * part, axis=1, keepdims=True)
        factor = lax.rsqrt(square_sum / width + epsilon)
        for c in range(units // 256):
            cols = slice(c * 256, (c + 1) * 256)
            gate_part = jnp.zeros((piece_rows, 256), jnp.float32)
            up_part = jnp.zeros((piece_rows, 256), jnp.float32)
            for k in range(n_tp):
                depth = slice(k * col_count, (k + 1) * col_count)
                part = rows[s, k]
                gate_part = gate_part + jnp.dot(
                    part, wg[depth, cols], preferred_element_type=jnp.float32
                )
                up_part = up_part + jnp.dot(
                    part, wu[depth, cols], preferred_element_type=jnp.float32
                )
            gate_part = gate_part * factor
            up_part = up_part * factor
            hidden[:, cols] = (gate_part / (1.0 + jnp.exp(-gate_part)) * up_part).astype(
                jnp.bfloat16
            )

        @pl.when(i + AHEAD < stages)
        def _():
            forward(i + AHEAD)

        @pl.when(i + 1 < stages)
        def _():
            after = unit_of(i + 1)
            x_copy(after).wait_recv()
            e_copy(after).start()

        for j in range(2):
            to_core[s, j] = jnp.dot(
                hidden[...], wd[j], preferred_element_type=jnp.float32
            ).astype(jnp.bfloat16)
            pc_copy(s, j).start()
        part = jnp.dot(hidden[...], wd[2], preferred_element_type=jnp.float32)
        own[i % (LAG + 1)] = jnp.dot(hidden[...], wd[3], preferred_element_type=jnp.float32)
        pc_copy(s, 0).wait_recv()
        to_chip[s] = (part + from_core[s, 0].astype(jnp.float32)).astype(jnp.bfloat16)
        px_copy(s).start()

        @pl.when(i >= LAG)
        def _():
            finish(i - LAG)

        return carry

    lax.fori_loop(0, stages, stage, 0)
    for i in range(stages - LAG, stages - 1):
        finish(i)

    slot_lanes = lax.broadcasted_iota(jnp.int32, (tok_count, piece_rows), 1).astype(
        jnp.float32
    )

    def unpack(i, h, values):
        pick = jnp.where(slot_lanes + h * piece_rows == place[:, i : i + 1], 1.0, 0.0)
        return jnp.dot(pick.astype(jnp.bfloat16), values, preferred_element_type=jnp.float32)

    mixed = jnp.zeros((tok_count, col_count), jnp.float32)
    for i in range(1, n_ep):
        taken = jnp.zeros((tok_count, col_count), jnp.float32)
        for h in range(cuts):
            r_copy(order[i], order[i], h).wait_recv()
            taken = taken + unpack(i, h, back[order[i] * cuts + h])
        mixed = mixed + weight[:, i : i + 1] * taken
    acc[...] = mixed

    def drain(pieces, sem):
        pltpu.make_async_remote_copy(
            src_ref=pieces,
            dst_ref=pieces,
            send_sem=sem,
            recv_sem=px_recv.at[0],
            device_id={"tp": across},
            device_id_type=MESH,
        ).wait_send()

    others = stages - cuts
    drain(packed.at[pl.ds(0, others)], z_send)
    drain(result.at[pl.ds(0, others)], r_send)
    drain(to_chip, x_send)
    drain(to_chip, d_send)
    drain(to_chip, e_send)
    drain(to_core, pc_send)

    finish(stages - 1)
    taken = jnp.zeros((tok_count, col_count), jnp.float32)
    for h in range(cuts):
        taken = taken + unpack(0, h, result[ep * cuts + h])
    out_ref[...] = (acc[...] + weight[:, 0:1] * taken).astype(jnp.bfloat16)
    drain(to_chip, px_send)


def fused(tokens, norm_gain, expert_ids, gate_weights, w_gate, w_up, w_down):
    tok_count, col_count = tokens.shape
    top_count = expert_ids.shape[1]
    n_ep = lax.axis_size("ep")
    n_tp = lax.axis_size("tp")
    cap = 3 * tok_count * top_count // (2 * n_ep)
    cuts = 2 if cap % 32 == 0 else 1
    stages, piece_rows = n_ep * cuts, cap // cuts
    width = norm_gain.shape[0]
    units = w_gate.shape[2]
    bf16 = jnp.bfloat16
    vmem = pl.BlockSpec(memory_space=pltpu.VMEM)
    anywhere = pl.BlockSpec(memory_space=pl.ANY)
    sems = pltpu.SemaphoreType.DMA
    return pl.pallas_call(
        functools.partial(layer_kernel, n_ep, cap, cuts),
        out_shape=jax.ShapeDtypeStruct((tok_count, col_count), bf16),
        in_specs=[anywhere] * 7,
        out_specs=vmem,
        scratch_shapes=[
            pltpu.VMEM((tok_count, col_count), bf16),
            pltpu.VMEM((top_count, tok_count), jnp.int32),
            pltpu.VMEM((top_count, tok_count), jnp.float32),
            pltpu.VMEM((1, width), jnp.float32),
            pltpu.VMEM((tok_count, col_count), jnp.float32),
            pltpu.VMEM((width, units), bf16),
            pltpu.VMEM((width, units), bf16),
            pltpu.VMEM((n_tp, units, col_count), bf16),
            pltpu.VMEM((stages, piece_rows, col_count), bf16),
            pltpu.VMEM((stages, n_tp, piece_rows, col_count), bf16),
            pltpu.VMEM((piece_rows, units), bf16),
            pltpu.VMEM((LAG + 1, piece_rows, col_count), jnp.float32),
            pltpu.VMEM((stages, 2, piece_rows, col_count), bf16),
            pltpu.VMEM((stages, 2, piece_rows, col_count), bf16),
        ]
        + [pltpu.VMEM((stages, piece_rows, col_count), bf16)] * 4
        + [sems((2 + n_tp,)), sems((4,))]
        + [sems, sems((stages,))] * 4
        + [sems, sems((stages, 2))]
        + [sems, sems((stages,))] * 2,
        compiler_params=pltpu.CompilerParams(
            collective_id=0, has_side_effects=True, vmem_limit_bytes=56 * 2**20
        ),
    )(
        tokens,
        expert_ids.T,
        gate_weights.T,
        norm_gain.reshape(1, width),
        w_gate,
        w_up,
        w_down,
    )


def on_device(tokens, norm_gain, expert_ids, gate_weights, w_gate, w_up, w_down):
    tok_count = tokens.shape[0]
    top_count = expert_ids.shape[1]
    expert_count = lax.axis_size("ep")
    capacity = 3 * tok_count * top_count // (2 * expert_count)
    model_width = norm_gain.shape[0]
    flat_ids = expert_ids.reshape(-1)
    onehot = (flat_ids[:, None] == jnp.arange(expert_count, dtype=jnp.int32)[None, :]).astype(
        jnp.int32
    )
    earlier = jnp.cumsum(onehot, axis=0) - onehot
    slot_index = jnp.sum(earlier * onehot, axis=1)
    dest_index = flat_ids * capacity + slot_index
    owner_index = jnp.arange(tok_count * top_count, dtype=jnp.int32) // top_count
    slot_token = (
        jnp.full((expert_count * capacity,), tok_count, jnp.int32).at[dest_index].set(owner_index)
    )
    tok_values = tokens.astype(jnp.float32)
    square_sum = lax.psum(jnp.sum(tok_values * tok_values, axis=1, keepdims=True), "tp")
    col_count = tokens.shape[1]
    gain_part = lax.dynamic_slice_in_dim(norm_gain, lax.axis_index("tp") * col_count, col_count)
    normed = (tok_values * lax.rsqrt(square_sum / model_width + epsilon) * gain_part).astype(
        jnp.bfloat16
    )
    buffer = jnp.take(normed, slot_token, axis=0, mode="fill", fill_value=0).reshape(
        expert_count, capacity, -1
    )
    received = lax.all_to_all(buffer, "ep", split_axis=0, concat_axis=0, tiled=True)
    source_count, item_count, col_count = received.shape
    tok_rows = received.reshape(-1, col_count)
    col_piece = lax.all_gather(tok_rows, "tp", axis=1, tiled=True)
    gate_rows = w_gate[0]
    up_rows = w_up[0]
    gate_part = jnp.dot(col_piece, gate_rows, preferred_element_type=jnp.float32)
    up_part = jnp.dot(col_piece, up_rows, preferred_element_type=jnp.float32)
    hidden = (jax.nn.silu(gate_part) * up_part).astype(jnp.bfloat16)
    partial_value = jnp.dot(hidden, w_down[0], preferred_element_type=jnp.float32)
    partial_value = partial_value.reshape(source_count, item_count, -1)
    summed = lax.psum_scatter(
        partial_value.astype(jnp.bfloat16), "tp", scatter_dimension=2, tiled=True
    )
    came_back = lax.all_to_all(summed, "ep", split_axis=0, concat_axis=0, tiled=True)
    picked = came_back.reshape(expert_count * capacity, -1)[dest_index].astype(jnp.float32)
    weighted = picked * gate_weights.reshape(-1)[:, None]
    return jnp.sum(weighted.reshape(tok_count, top_count, -1), axis=1).astype(jnp.bfloat16)


def solution(mesh):
    return jax.shard_map(
        fused if mesh.shape["tp"] == 4 else on_device,
        mesh=mesh,
        in_specs=(
            P(("grp", "ep"), "tp"),
            P(),
            P(("grp", "ep"), None),
            P(("grp", "ep"), None),
            P("ep", None, "tp"),
            P("ep", None, "tp"),
            P("ep", "tp", None),
        ),
        out_specs=P(("grp", "ep"), "tp"),
        check_vma=False,
    )
```

```python
import functools

import jax
import jax.numpy as jnp
from jax import lax
from jax.experimental import pallas as pl
from jax.experimental.pallas import tpu as pltpu
from jax.sharding import PartitionSpec as P

epsilon = 1e-06
AHEAD = 2
LAG = 2
MESH = pl.DeviceIdType.MESH


def nearest_first(count):
    table = []
    for e in range(count):
        mirrored = 1 if 2 * e < count else -1
        table.append(sorted(range(count), key=lambda s: (abs(s - e), mirrored * s)))
    return table


def mirrored(units, count):
    return [(count - 1 - s, h) for s, h in units]


def unit_order(n_ep, cuts):
    if (n_ep, cuts) == (4, 2):
        outer = [(0, 1), (1, 0), (2, 1), (3, 0), (3, 1), (2, 0), (1, 1), (0, 0)]
        inner = [(1, 1), (3, 0), (0, 1), (2, 0), (3, 1), (0, 0), (2, 1), (1, 0)]
        both = [outer, inner, mirrored(inner, 4), mirrored(outer, 4)]
    else:
        both = [
            [(row[0], h) for h in range(cuts - 1)]
            + [(s, h) for s in row[1:] for h in range(cuts)]
            + [(row[0], cuts - 1)]
            for row in nearest_first(n_ep)
        ]
    return [[s * cuts + h for s, h in row] for row in both]


def send_order(n_ep, cuts):
    if (n_ep, cuts) == (4, 2):
        outer = [(2, 0), (1, 1), (1, 0), (3, 0), (2, 1), (3, 1)]
        inner = [(0, 0), (3, 1), (2, 0), (2, 1), (3, 0), (0, 1)]
        both = [outer, inner, mirrored(inner, 4), mirrored(outer, 4)]
    else:
        both = [
            [(s, h) for s in row[1:] for h in range(cuts)] for row in nearest_first(n_ep)
        ]
    return [[s * cuts + h for s, h in row] for row in both]


def first_named(units, cuts):
    return list(dict.fromkeys(unit // cuts for unit in units))


def pick_row(table, row):
    picked = []
    for column in range(len(table[0])):
        value = jnp.int32(table[0][column])
        for r in range(1, len(table)):
            value = jnp.where(row == r, table[r][column], value)
        picked.append(value)
    return picked


def entry_of(entries, index):
    value = entries[0]
    for c in range(1, len(entries)):
        value = jnp.where(index == c, entries[c], value)
    return value


def layer_kernel(
    n_ep,
    cap,
    cuts,
    tok_hbm,
    ids_hbm,
    gate_hbm,
    gain_hbm,
    wg_ref,
    wu_ref,
    wd_ref,
    out_ref,
    tok_ref,
    ids_ref,
    gate_ref,
    gain_ref,
    acc,
    wg,
    wu,
    wd,
    packed,
    rows,
    hidden,
    own,
    to_core,
    from_core,
    to_chip,
    from_chip,
    result,
    back,
    w_sem,
    i_sem,
    z_send,
    z_recv,
    x_send,
    x_recv,
    d_send,
    d_recv,
    e_send,
    e_recv,
    pc_send,
    pc_recv,
    px_send,
    px_recv,
    r_send,
    r_recv,
):
    tok_count, col_count = tok_ref.shape
    top_count = ids_ref.shape[0]
    n_tp = rows.shape[1]
    units = wg.shape[1]
    width = n_tp * col_count
    ep = lax.axis_index("ep")
    tp = lax.axis_index("tp")
    core = tp % 2
    sibling = tp + 1 - 2 * core
    across = (tp + 2) % n_tp
    side = tp // 2
    barrier = pltpu.get_barrier_semaphore()
    for step in range(1, n_ep):
        pl.semaphore_signal(
            barrier, inc=1, device_id={"ep": (ep + step) % n_ep}, device_id_type=MESH
        )
    for peer in (sibling, across):
        pl.semaphore_signal(barrier, inc=1, device_id={"tp": peer}, device_id_type=MESH)

    inputs = [
        pltpu.make_async_copy(source, target, i_sem.at[n])
        for n, (source, target) in enumerate(
            [
                (ids_hbm, ids_ref),
                (gate_hbm, gate_ref),
                (tok_hbm, tok_ref),
                (gain_hbm, gain_ref),
            ]
        )
    ]
    for copy in inputs:
        copy.start()

    order = [ep] + pick_row([first_named(row, cuts) for row in send_order(n_ep, cuts)], ep)
    turns = pick_row(unit_order(n_ep, cuts), ep)
    sends = pick_row(send_order(n_ep, cuts), ep)

    weights = [
        pltpu.make_async_copy(wg_ref.at[0], wg, w_sem.at[0]),
        pltpu.make_async_copy(wu_ref.at[0], wu, w_sem.at[1]),
    ]
    piece_of = [
        (1 - side) * 2 + 1 - core,
        side * 2 + 1 - core,
        (1 - side) * 2 + core,
        side * 2 + core,
    ]
    for j, piece in enumerate(piece_of):
        cols = pl.ds(pl.multiple_of(piece * col_count, col_count), col_count)
        weights.append(
            pltpu.make_async_copy(wd_ref.at[0, :, cols], wd.at[j], w_sem.at[2 + j])
        )
    inputs[0].wait()
    inputs[1].wait()
    lane = lax.broadcasted_iota(jnp.int32, (tok_count, 128), 1)
    lane_expert = jnp.full((tok_count, 128), -1, jnp.int32)
    for i in range(n_ep):
        lane_expert = jnp.where(lane == i, order[i], lane_expert)
    ids = ids_ref[...].astype(jnp.float32).T
    gates = gate_ref[...].T
    lane_expert = lane_expert.astype(jnp.float32)
    named = jnp.zeros((tok_count, 128), jnp.float32)
    weight = jnp.zeros((tok_count, 128), jnp.float32)
    for k in range(top_count):
        hit = ids[:, k : k + 1] == lane_expert
        named = named + jnp.where(hit, 1.0, 0.0)
        weight = weight + jnp.where(hit, gates[:, k : k + 1], 0.0)
    before = jnp.where(
        lax.broadcasted_iota(jnp.int32, (tok_count, tok_count), 1)
        < lax.broadcasted_iota(jnp.int32, (tok_count, tok_count), 0),
        1.0,
        0.0,
    ).astype(jnp.bfloat16)
    place = jnp.dot(before, named.astype(jnp.bfloat16), preferred_element_type=jnp.float32)
    place = jnp.where(named > 0.0, place, -1.0)
    place_t = place.T
    slot_rows = lax.broadcasted_iota(jnp.int32, (cap, tok_count), 0).astype(jnp.float32)

    def pack(i):
        pick = jnp.where(slot_rows == place_t[i : i + 1, :], 1.0, 0.0).astype(jnp.bfloat16)
        return jnp.dot(pick, tok_ref[...], preferred_element_type=jnp.float32).astype(
            jnp.bfloat16
        )

    def z_copy(here, there, h):
        return pltpu.make_async_remote_copy(
            src_ref=packed.at[there * cuts + h],
            dst_ref=rows.at[here * cuts + h, tp],
            send_sem=z_send,
            recv_sem=z_recv.at[here * cuts + h],
            device_id={"ep": there},
            device_id_type=MESH,
        )

    def x_copy(i):
        return pltpu.make_async_remote_copy(
            src_ref=rows.at[i, tp],
            dst_ref=rows.at[i, tp],
            send_sem=x_send,
            recv_sem=x_recv.at[i],
            device_id={"tp": across},
            device_id_type=MESH,
        )

    def d_copy(i):
        return pltpu.make_async_remote_copy(
            src_ref=rows.at[i, tp],
            dst_ref=rows.at[i, tp],
            send_sem=d_send,
            recv_sem=d_recv.at[i],
            device_id={"tp": sibling},
            device_id_type=MESH,
        )

    def e_copy(i):
        return pltpu.make_async_remote_copy(
            src_ref=rows.at[i, across],
            dst_ref=rows.at[i, across],
            send_sem=e_send,
            recv_sem=e_recv.at[i],
            device_id={"tp": sibling},
            device_id_type=MESH,
        )

    def pc_copy(i, j):
        return pltpu.make_async_remote_copy(
            src_ref=to_core.at[i, j],
            dst_ref=from_core.at[i, j],
            send_sem=pc_send,
            recv_sem=pc_recv.at[i, j],
            device_id={"tp": sibling},
            device_id_type=MESH,
        )

    def px_copy(i):
        return pltpu.make_async_remote_copy(
            src_ref=to_chip.at[i],
            dst_ref=from_chip.at[i],
            send_sem=px_send,
            recv_sem=px_recv.at[i],
            device_id={"tp": across},
            device_id_type=MESH,
        )

    def r_copy(here, there, h):
        return pltpu.make_async_remote_copy(
            src_ref=result.at[there * cuts + h],
            dst_ref=back.at[here * cuts + h],
            send_sem=r_send,
            recv_sem=r_recv.at[here * cuts + h],
            device_id={"ep": there},
            device_id_type=MESH,
        )

    piece_rows = cap // cuts
    stages = n_ep * cuts
    inputs[2].wait()
    for copy in weights[:2]:
        copy.start()
    values = pack(0)
    for h in range(cuts):
        rows[ep * cuts + h, tp] = values[h * piece_rows : (h + 1) * piece_rows]

    def unit_of(i):
        return turns[i] if isinstance(i, int) else entry_of(turns, i)

    def spread(s):
        x_copy(s).start()
        d_copy(s).start()

    def forward(i):
        s = unit_of(i)

        @pl.when(s // cuts != ep)
        def _():
            z_copy(s // cuts, s // cuts, s % cuts).wait_recv()
            spread(s)

    pl.semaphore_wait(barrier, n_ep + 1)
    for h in range(cuts):
        spread(ep * cuts + h)
    for i in range(1, n_ep):
        values = pack(i)
        for h in range(cuts):
            packed[order[i] * cuts + h] = values[h * piece_rows : (h + 1) * piece_rows]
        for unit in sends[i - 1 :] if i + 1 == n_ep else sends[i - 1 : i]:
            z_copy(ep, unit // cuts, unit % cuts).start()
    inputs[3].wait()
    for copy in weights[:2]:
        copy.wait()
    for copy in weights[2:]:
        copy.start()

    def scale(i, carry):
        block = pl.ds(pl.multiple_of(i * 128, 128), 128)
        gain = jnp.broadcast_to(gain_ref[:, block], (128, 128)).T
        for matrix in (wg, wu):
            for c in range(units // 128):
                cols = slice(c * 128, (c + 1) * 128)
                matrix[block, cols] = (matrix[block, cols].astype(jnp.float32) * gain).astype(
                    jnp.bfloat16
                )
        return carry

    lax.fori_loop(0, width // 128, scale, 0, unroll=2)

    def finish(i):
        s = unit_of(i)
        pc_copy(s, 1).wait_recv()
        total = own[i % (LAG + 1)] + from_core[s, 1].astype(jnp.float32)
        px_copy(s).wait_recv()
        total = total + from_chip[s].astype(jnp.float32)
        result[s] = total.astype(jnp.bfloat16)

        @pl.when(s // cuts != ep)
        def _():
            r_copy(ep, s // cuts, s % cuts).start()

    for i in range(1, AHEAD):
        forward(i)
    x_copy(unit_of(0)).wait_recv()
    e_copy(unit_of(0)).start()
    for copy in weights[2:]:
        copy.wait()

    def stage(i, carry):
        s = unit_of(i)
        d_copy(s).wait_recv()
        e_copy(s).wait_recv()
        square_sum = jnp.zeros((piece_rows, 1), jnp.float32)
        for k in range(n_tp):
            part = rows[s, k].astype(jnp.float32)
            square_sum = square_sum + jnp.sum(part * part, axis=1, keepdims=True)
        factor = lax.rsqrt(square_sum / width + epsilon)
        for c in range(units // 256):
            cols = slice(c * 256, (c + 1) * 256)
            gate_part = jnp.zeros((piece_rows, 256), jnp.float32)
            up_part = jnp.zeros((piece_rows, 256), jnp.float32)
            for k in range(n_tp):
                depth = slice(k * col_count, (k + 1) * col_count)
                part = rows[s, k]
                gate_part = gate_part + jnp.dot(
                    part, wg[depth, cols], preferred_element_type=jnp.float32
                )
                up_part = up_part + jnp.dot(
                    part, wu[depth, cols], preferred_element_type=jnp.float32
                )
            gate_part = gate_part * factor
            up_part = up_part * factor
            hidden[:, cols] = (gate_part / (1.0 + jnp.exp(-gate_part)) * up_part).astype(
                jnp.bfloat16
            )

        @pl.when(i >= LAG)
        def _():
            finish(i - LAG)

        @pl.when(i + AHEAD < stages)
        def _():
            forward(i + AHEAD)

        to_core[s, 0] = jnp.dot(
            hidden[...], wd[0], preferred_element_type=jnp.float32
        ).astype(jnp.bfloat16)
        pc_copy(s, 0).start()
        to_core[s, 1] = jnp.dot(
            hidden[...], wd[1], preferred_element_type=jnp.float32
        ).astype(jnp.bfloat16)
        part = jnp.dot(hidden[...], wd[2], preferred_element_type=jnp.float32)
        own[i % (LAG + 1)] = jnp.dot(hidden[...], wd[3], preferred_element_type=jnp.float32)
        pc_copy(s, 1).start()
        pc_copy(s, 0).wait_recv()
        to_chip[s] = (part + from_core[s, 0].astype(jnp.float32)).astype(jnp.bfloat16)
        px_copy(s).start()

        @pl.when(i + 1 < stages)
        def _():
            after = unit_of(i + 1)
            x_copy(after).wait_recv()
            e_copy(after).start()

        return carry

    lax.fori_loop(0, stages, stage, 0)
    for i in range(stages - LAG, stages - 1):
        finish(i)

    slot_lanes = lax.broadcasted_iota(jnp.int32, (tok_count, piece_rows), 1).astype(
        jnp.float32
    )

    def unpack(i, h, values):
        pick = jnp.where(slot_lanes + h * piece_rows == place[:, i : i + 1], 1.0, 0.0)
        return jnp.dot(pick.astype(jnp.bfloat16), values, preferred_element_type=jnp.float32)

    mixed = jnp.zeros((tok_count, col_count), jnp.float32)
    for i in range(1, n_ep):
        taken = jnp.zeros((tok_count, col_count), jnp.float32)
        for h in range(cuts):
            r_copy(order[i], order[i], h).wait_recv()
            taken = taken + unpack(i, h, back[order[i] * cuts + h])
        mixed = mixed + weight[:, i : i + 1] * taken
    acc[...] = mixed

    def drain(pieces, sem):
        pltpu.make_async_remote_copy(
            src_ref=pieces,
            dst_ref=pieces,
            send_sem=sem,
            recv_sem=px_recv.at[0],
            device_id={"tp": across},
            device_id_type=MESH,
        ).wait_send()

    others = stages - cuts
    drain(packed.at[pl.ds(0, others)], z_send)
    drain(result.at[pl.ds(0, others)], r_send)
    drain(to_chip, x_send)
    drain(to_chip, d_send)
    drain(to_chip, e_send)
    drain(to_core, pc_send)

    finish(stages - 1)
    taken = jnp.zeros((tok_count, col_count), jnp.float32)
    for h in range(cuts):
        taken = taken + unpack(0, h, result[ep * cuts + h])
    out_ref[...] = (acc[...] + weight[:, 0:1] * taken).astype(jnp.bfloat16)
    drain(to_chip, px_send)


def fused(tokens, norm_gain, expert_ids, gate_weights, w_gate, w_up, w_down):
    tok_count, col_count = tokens.shape
    top_count = expert_ids.shape[1]
    n_ep = lax.axis_size("ep")
    n_tp = lax.axis_size("tp")
    cap = 3 * tok_count * top_count // (2 * n_ep)
    cuts = 2 if cap % 32 == 0 else 1
    stages, piece_rows = n_ep * cuts, cap // cuts
    width = norm_gain.shape[0]
    units = w_gate.shape[2]
    bf16 = jnp.bfloat16
    vmem = pl.BlockSpec(memory_space=pltpu.VMEM)
    anywhere = pl.BlockSpec(memory_space=pl.ANY)
    sems = pltpu.SemaphoreType.DMA
    return pl.pallas_call(
        functools.partial(layer_kernel, n_ep, cap, cuts),
        out_shape=jax.ShapeDtypeStruct((tok_count, col_count), bf16),
        in_specs=[anywhere] * 7,
        out_specs=vmem,
        scratch_shapes=[
            pltpu.VMEM((tok_count, col_count), bf16),
            pltpu.VMEM((top_count, tok_count), jnp.int32),
            pltpu.VMEM((top_count, tok_count), jnp.float32),
            pltpu.VMEM((1, width), jnp.float32),
            pltpu.VMEM((tok_count, col_count), jnp.float32),
            pltpu.VMEM((width, units), bf16),
            pltpu.VMEM((width, units), bf16),
            pltpu.VMEM((n_tp, units, col_count), bf16),
            pltpu.VMEM((stages, piece_rows, col_count), bf16),
            pltpu.VMEM((stages, n_tp, piece_rows, col_count), bf16),
            pltpu.VMEM((piece_rows, units), bf16),
            pltpu.VMEM((LAG + 1, piece_rows, col_count), jnp.float32),
            pltpu.VMEM((stages, 2, piece_rows, col_count), bf16),
            pltpu.VMEM((stages, 2, piece_rows, col_count), bf16),
        ]
        + [pltpu.VMEM((stages, piece_rows, col_count), bf16)] * 4
        + [sems((2 + n_tp,)), sems((4,))]
        + [sems, sems((stages,))] * 4
        + [sems, sems((stages, 2))]
        + [sems, sems((stages,))] * 2,
        compiler_params=pltpu.CompilerParams(
            collective_id=0, has_side_effects=True, vmem_limit_bytes=40 * 2**20
        ),
    )(
        *(
            pltpu.with_memory_space_constraint(operand, pltpu.HBM)
            for operand in (
                tokens,
                expert_ids.T,
                gate_weights.T,
                norm_gain.reshape(1, width),
                w_gate,
                w_up,
                w_down,
            )
        )
    )


def on_device(tokens, norm_gain, expert_ids, gate_weights, w_gate, w_up, w_down):
    tok_count = tokens.shape[0]
    top_count = expert_ids.shape[1]
    expert_count = lax.axis_size("ep")
    capacity = 3 * tok_count * top_count // (2 * expert_count)
    model_width = norm_gain.shape[0]
    flat_ids = expert_ids.reshape(-1)
    onehot = (flat_ids[:, None] == jnp.arange(expert_count, dtype=jnp.int32)[None, :]).astype(
        jnp.int32
    )
    earlier = jnp.cumsum(onehot, axis=0) - onehot
    slot_index = jnp.sum(earlier * onehot, axis=1)
    dest_index = flat_ids * capacity + slot_index
    owner_index = jnp.arange(tok_count * top_count, dtype=jnp.int32) // top_count
    slot_token = (
        jnp.full((expert_count * capacity,), tok_count, jnp.int32).at[dest_index].set(owner_index)
    )
    tok_values = tokens.astype(jnp.float32)
    square_sum = lax.psum(jnp.sum(tok_values * tok_values, axis=1, keepdims=True), "tp")
    col_count = tokens.shape[1]
    gain_part = lax.dynamic_slice_in_dim(norm_gain, lax.axis_index("tp") * col_count, col_count)
    normed = (tok_values * lax.rsqrt(square_sum / model_width + epsilon) * gain_part).astype(
        jnp.bfloat16
    )
    buffer = jnp.take(normed, slot_token, axis=0, mode="fill", fill_value=0).reshape(
        expert_count, capacity, -1
    )
    received = lax.all_to_all(buffer, "ep", split_axis=0, concat_axis=0, tiled=True)
    source_count, item_count, col_count = received.shape
    tok_rows = received.reshape(-1, col_count)
    col_piece = lax.all_gather(tok_rows, "tp", axis=1, tiled=True)
    gate_rows = w_gate[0]
    up_rows = w_up[0]
    gate_part = jnp.dot(col_piece, gate_rows, preferred_element_type=jnp.float32)
    up_part = jnp.dot(col_piece, up_rows, preferred_element_type=jnp.float32)
    hidden = (jax.nn.silu(gate_part) * up_part).astype(jnp.bfloat16)
    partial_value = jnp.dot(hidden, w_down[0], preferred_element_type=jnp.float32)
    partial_value = partial_value.reshape(source_count, item_count, -1)
    summed = lax.psum_scatter(
        partial_value.astype(jnp.bfloat16), "tp", scatter_dimension=2, tiled=True
    )
    came_back = lax.all_to_all(summed, "ep", split_axis=0, concat_axis=0, tiled=True)
    picked = came_back.reshape(expert_count * capacity, -1)[dest_index].astype(jnp.float32)
    weighted = picked * gate_weights.reshape(-1)[:, None]
    return jnp.sum(weighted.reshape(tok_count, top_count, -1), axis=1).astype(jnp.bfloat16)


def solution(mesh):
    return jax.shard_map(
        fused if mesh.shape["tp"] == 4 else on_device,
        mesh=mesh,
        in_specs=(
            P(("grp", "ep"), "tp"),
            P(),
            P(("grp", "ep"), None),
            P(("grp", "ep"), None),
            P("ep", None, "tp"),
            P("ep", None, "tp"),
            P("ep", "tp", None),
        ),
        out_specs=P(("grp", "ep"), "tp"),
        check_vma=False,
    )
```

```python
import functools

import jax
import jax.numpy as jnp
from jax import lax
from jax.experimental import pallas as pl
from jax.experimental.pallas import tpu as pltpu
from jax.sharding import PartitionSpec as P

epsilon = 1e-06
AHEAD = 2
LAG = 2
MESH = pl.DeviceIdType.MESH


def nearest_first(count):
    table = []
    for e in range(count):
        mirrored = 1 if 2 * e < count else -1
        table.append(sorted(range(count), key=lambda s: (abs(s - e), mirrored * s)))
    return table


def unit_order(n_ep, cuts):
    if (n_ep, cuts) == (4, 2):
        rows = [
            [(0, 1), (1, 0), (2, 1), (3, 0), (3, 1), (2, 0), (1, 1), (0, 0)],
            [(1, 1), (3, 0), (0, 1), (2, 0), (3, 1), (0, 0), (2, 1), (1, 0)],
            [(2, 1), (3, 1), (0, 0), (0, 1), (1, 0), (1, 1), (3, 0), (2, 0)],
            [(3, 1), (2, 0), (1, 1), (0, 0), (0, 1), (1, 0), (2, 1), (3, 0)],
        ]
    else:
        rows = [
            [(row[0], h) for h in range(cuts - 1)]
            + [(s, h) for s in row[1:] for h in range(cuts)]
            + [(row[0], cuts - 1)]
            for row in nearest_first(n_ep)
        ]
    return [[s * cuts + h for s, h in row] for row in rows]


def send_order(n_ep, cuts):
    if (n_ep, cuts) == (4, 2):
        rows = [
            [(2, 0), (1, 1), (1, 0), (3, 0), (2, 1), (3, 1)],
            [(0, 0), (3, 1), (2, 1), (3, 0), (2, 0), (0, 1)],
            [(0, 1), (3, 0), (1, 0), (1, 1), (0, 0), (3, 1)],
            [(1, 0), (2, 1), (2, 0), (0, 0), (1, 1), (0, 1)],
        ]
    else:
        rows = [
            [(s, h) for s in row[1:] for h in range(cuts)] for row in nearest_first(n_ep)
        ]
    return [[s * cuts + h for s, h in row] for row in rows]


def first_named(units, cuts):
    return list(dict.fromkeys(unit // cuts for unit in units))


def pick_row(table, row):
    picked = []
    for column in range(len(table[0])):
        value = jnp.int32(table[0][column])
        for r in range(1, len(table)):
            value = jnp.where(row == r, table[r][column], value)
        picked.append(value)
    return picked


def entry_of(entries, index):
    value = entries[0]
    for c in range(1, len(entries)):
        value = jnp.where(index == c, entries[c], value)
    return value


def layer_kernel(
    n_ep,
    cap,
    cuts,
    tok_hbm,
    ids_hbm,
    gate_hbm,
    gain_hbm,
    wg_ref,
    wu_ref,
    wd_ref,
    out_ref,
    tok_ref,
    ids_ref,
    gate_ref,
    gain_ref,
    acc,
    wg,
    wu,
    wd,
    packed,
    rows,
    hidden,
    own,
    to_core,
    from_core,
    to_chip,
    from_chip,
    result,
    back,
    w_sem,
    i_sem,
    z_send,
    z_recv,
    x_send,
    x_recv,
    d_send,
    d_recv,
    e_send,
    e_recv,
    pc_send,
    pc_recv,
    px_send,
    px_recv,
    r_send,
    r_recv,
):
    tok_count, col_count = tok_ref.shape
    top_count = ids_ref.shape[0]
    n_tp = rows.shape[1]
    units = wg.shape[1]
    width = n_tp * col_count
    ep = lax.axis_index("ep")
    tp = lax.axis_index("tp")
    core = tp % 2
    sibling = tp + 1 - 2 * core
    across = (tp + 2) % n_tp
    side = tp // 2
    barrier = pltpu.get_barrier_semaphore()
    for step in range(1, n_ep):
        pl.semaphore_signal(
            barrier, inc=1, device_id={"ep": (ep + step) % n_ep}, device_id_type=MESH
        )
    for peer in (sibling, across):
        pl.semaphore_signal(barrier, inc=1, device_id={"tp": peer}, device_id_type=MESH)

    inputs = [
        pltpu.make_async_copy(source, target, i_sem.at[n])
        for n, (source, target) in enumerate(
            [
                (ids_hbm, ids_ref),
                (gate_hbm, gate_ref),
                (tok_hbm, tok_ref),
                (gain_hbm, gain_ref),
            ]
        )
    ]
    for copy in inputs:
        copy.start()

    order = [ep] + pick_row([first_named(row, cuts) for row in send_order(n_ep, cuts)], ep)
    turns = pick_row(unit_order(n_ep, cuts), ep)
    sends = pick_row(send_order(n_ep, cuts), ep)

    weights = [
        pltpu.make_async_copy(wg_ref.at[0], wg, w_sem.at[0]),
        pltpu.make_async_copy(wu_ref.at[0], wu, w_sem.at[1]),
    ]
    piece_of = [
        (1 - side) * 2 + 1 - core,
        side * 2 + 1 - core,
        (1 - side) * 2 + core,
        side * 2 + core,
    ]
    for j, piece in enumerate(piece_of):
        cols = pl.ds(pl.multiple_of(piece * col_count, col_count), col_count)
        weights.append(
            pltpu.make_async_copy(wd_ref.at[0, :, cols], wd.at[j], w_sem.at[2 + j])
        )
    inputs[0].wait()
    inputs[1].wait()
    columns = -(-n_ep // 16) * 16
    column = lax.broadcasted_iota(jnp.int32, (columns, tok_count), 0)
    column_expert = jnp.full((columns, tok_count), -1, jnp.int32)
    for i in range(n_ep):
        column_expert = jnp.where(column == i, order[i], column_expert)
    named = jnp.zeros((columns, tok_count), jnp.float32)
    weight_t = jnp.zeros((columns, tok_count), jnp.float32)
    for k in range(top_count):
        hit = ids_ref[k : k + 1, :] == column_expert
        named = named + jnp.where(hit, 1.0, 0.0)
        weight_t = weight_t + jnp.where(hit, gate_ref[k : k + 1, :], 0.0)
    before = jnp.where(
        lax.broadcasted_iota(jnp.int32, (tok_count, tok_count), 0)
        < lax.broadcasted_iota(jnp.int32, (tok_count, tok_count), 1),
        1.0,
        0.0,
    ).astype(jnp.bfloat16)
    place_t = jnp.dot(named.astype(jnp.bfloat16), before, preferred_element_type=jnp.float32)
    place_t = jnp.where(named > 0.0, place_t, -1.0)
    slot_rows = lax.broadcasted_iota(jnp.int32, (cap, tok_count), 0).astype(jnp.float32)

    def pack(i):
        pick = jnp.where(slot_rows == place_t[i : i + 1, :], 1.0, 0.0).astype(jnp.bfloat16)
        return jnp.dot(pick, tok_ref[...], preferred_element_type=jnp.float32).astype(
            jnp.bfloat16
        )

    def z_copy(here, there, h):
        return pltpu.make_async_remote_copy(
            src_ref=packed.at[there * cuts + h],
            dst_ref=rows.at[here * cuts + h, tp],
            send_sem=z_send,
            recv_sem=z_recv.at[here * cuts + h],
            device_id={"ep": there},
            device_id_type=MESH,
        )

    def x_copy(i):
        return pltpu.make_async_remote_copy(
            src_ref=rows.at[i, tp],
            dst_ref=rows.at[i, tp],
            send_sem=x_send,
            recv_sem=x_recv.at[i],
            device_id={"tp": across},
            device_id_type=MESH,
        )

    def d_copy(i):
        return pltpu.make_async_remote_copy(
            src_ref=rows.at[i, tp],
            dst_ref=rows.at[i, tp],
            send_sem=d_send,
            recv_sem=d_recv.at[i],
            device_id={"tp": sibling},
            device_id_type=MESH,
        )

    def e_copy(i):
        return pltpu.make_async_remote_copy(
            src_ref=rows.at[i, across],
            dst_ref=rows.at[i, across],
            send_sem=e_send,
            recv_sem=e_recv.at[i],
            device_id={"tp": sibling},
            device_id_type=MESH,
        )

    def pc_copy(i, j):
        return pltpu.make_async_remote_copy(
            src_ref=to_core.at[i, j],
            dst_ref=from_core.at[i, j],
            send_sem=pc_send,
            recv_sem=pc_recv.at[i, j],
            device_id={"tp": sibling},
            device_id_type=MESH,
        )

    def px_copy(i):
        return pltpu.make_async_remote_copy(
            src_ref=to_chip.at[i],
            dst_ref=from_chip.at[i],
            send_sem=px_send,
            recv_sem=px_recv.at[i],
            device_id={"tp": across},
            device_id_type=MESH,
        )

    def r_copy(here, there, h):
        return pltpu.make_async_remote_copy(
            src_ref=result.at[there * cuts + h],
            dst_ref=back.at[here * cuts + h],
            send_sem=r_send,
            recv_sem=r_recv.at[here * cuts + h],
            device_id={"ep": there},
            device_id_type=MESH,
        )

    piece_rows = cap // cuts
    stages = n_ep * cuts
    inputs[2].wait()
    for copy in weights[:2]:
        copy.start()
    values = pack(0)
    for h in range(cuts):
        rows[ep * cuts + h, tp] = values[h * piece_rows : (h + 1) * piece_rows]

    def unit_of(i):
        return turns[i] if isinstance(i, int) else entry_of(turns, i)

    def spread(s):
        x_copy(s).start()
        d_copy(s).start()

    def forward(i):
        s = unit_of(i)

        @pl.when(s // cuts != ep)
        def _():
            z_copy(s // cuts, s // cuts, s % cuts).wait_recv()
            spread(s)

    pl.semaphore_wait(barrier, n_ep + 1)
    for h in range(cuts):
        spread(ep * cuts + h)
    for i in range(1, n_ep):
        values = pack(i)
        for h in range(cuts):
            packed[order[i] * cuts + h] = values[h * piece_rows : (h + 1) * piece_rows]
        for unit in sends[i - 1 :] if i + 1 == n_ep else sends[i - 1 : i]:
            z_copy(ep, unit // cuts, unit % cuts).start()
    inputs[3].wait()
    for copy in weights[:2]:
        copy.wait()
    for copy in weights[2:]:
        copy.start()

    def scale(i, carry):
        block = pl.ds(pl.multiple_of(i * 128, 128), 128)
        gain = jnp.broadcast_to(gain_ref[:, block], (128, 128)).T
        for matrix in (wg, wu):
            for c in range(units // 128):
                cols = slice(c * 128, (c + 1) * 128)
                matrix[block, cols] = (matrix[block, cols].astype(jnp.float32) * gain).astype(
                    jnp.bfloat16
                )
        return carry

    lax.fori_loop(0, width // 128, scale, 0, unroll=2)

    def finish(i):
        s = unit_of(i)
        pc_copy(s, 1).wait_recv()
        total = own[i % (LAG + 1)] + from_core[s, 1].astype(jnp.float32)
        px_copy(s).wait_recv()
        total = total + from_chip[s].astype(jnp.float32)
        result[s] = total.astype(jnp.bfloat16)

        @pl.when(s // cuts != ep)
        def _():
            r_copy(ep, s // cuts, s % cuts).start()

    for i in range(1, AHEAD):
        forward(i)
    x_copy(unit_of(0)).wait_recv()
    e_copy(unit_of(0)).start()
    for copy in weights[2:]:
        copy.wait()

    def stage(i, carry):
        s = unit_of(i)
        d_copy(s).wait_recv()
        e_copy(s).wait_recv()
        square_sum = jnp.zeros((piece_rows, 1), jnp.float32)
        for k in range(n_tp):
            part = rows[s, k].astype(jnp.float32)
            square_sum = square_sum + jnp.sum(part * part, axis=1, keepdims=True)
        factor = lax.rsqrt(square_sum / width + epsilon)
        for c in range(units // 256):
            cols = slice(c * 256, (c + 1) * 256)
            gate_part = jnp.zeros((piece_rows, 256), jnp.float32)
            up_part = jnp.zeros((piece_rows, 256), jnp.float32)
            for k in range(n_tp):
                depth = slice(k * col_count, (k + 1) * col_count)
                part = rows[s, k]
                gate_part = gate_part + jnp.dot(
                    part, wg[depth, cols], preferred_element_type=jnp.float32
                )
                up_part = up_part + jnp.dot(
                    part, wu[depth, cols], preferred_element_type=jnp.float32
                )
            gate_part = gate_part * factor
            up_part = up_part * factor
            hidden[:, cols] = (gate_part / (1.0 + jnp.exp(-gate_part)) * up_part).astype(
                jnp.bfloat16
            )

        @pl.when(i >= LAG)
        def _():
            finish(i - LAG)

        @pl.when(i + AHEAD < stages)
        def _():
            forward(i + AHEAD)

        to_core[s, 0] = jnp.dot(
            hidden[...], wd[0], preferred_element_type=jnp.float32
        ).astype(jnp.bfloat16)
        pc_copy(s, 0).start()
        to_core[s, 1] = jnp.dot(
            hidden[...], wd[1], preferred_element_type=jnp.float32
        ).astype(jnp.bfloat16)
        part = jnp.dot(hidden[...], wd[2], preferred_element_type=jnp.float32)
        own[i % (LAG + 1)] = jnp.dot(hidden[...], wd[3], preferred_element_type=jnp.float32)
        pc_copy(s, 1).start()

        @pl.when(i + 2 < stages)
        def _():
            after = unit_of(i + 1)
            x_copy(after).wait_recv()
            e_copy(after).start()

        @pl.when(i == 1)
        def _():
            x_copy(unit_of(stages - 1)).wait_recv()
            e_copy(unit_of(stages - 1)).start()

        pc_copy(s, 0).wait_recv()
        to_chip[s] = (part + from_core[s, 0].astype(jnp.float32)).astype(jnp.bfloat16)
        px_copy(s).start()

        return carry

    lax.fori_loop(0, stages, stage, 0)
    for i in range(stages - LAG, stages - 1):
        finish(i)

    slot_lanes = lax.broadcasted_iota(jnp.int32, (tok_count, piece_rows), 1).astype(
        jnp.float32
    )

    place = place_t.T
    weight = weight_t.T

    def unpack(i, h, values):
        start = jnp.asarray(h * piece_rows, jnp.int32).astype(jnp.float32)
        pick = jnp.where(slot_lanes + start == place[:, i : i + 1], 1.0, 0.0)
        return jnp.dot(pick.astype(jnp.bfloat16), values, preferred_element_type=jnp.float32)

    mixed = jnp.zeros((tok_count, col_count), jnp.float32)
    for i in range(1, n_ep):
        taken = jnp.zeros((tok_count, col_count), jnp.float32)
        for h in range(cuts):
            r_copy(order[i], order[i], h).wait_recv()
            taken = taken + unpack(i, h, back[order[i] * cuts + h])
        mixed = mixed + weight[:, i : i + 1] * taken
    last = turns[stages - 1] % cuts
    for step in range(1, cuts):
        h = (last + step) % cuts
        mixed = mixed + weight[:, 0:1] * unpack(0, h, result[ep * cuts + h])
    acc[...] = mixed

    def drain(pieces, sem):
        pltpu.make_async_remote_copy(
            src_ref=pieces,
            dst_ref=pieces,
            send_sem=sem,
            recv_sem=px_recv.at[0],
            device_id={"tp": across},
            device_id_type=MESH,
        ).wait_send()

    others = stages - cuts
    drain(packed.at[pl.ds(0, others)], z_send)
    drain(result.at[pl.ds(0, others)], r_send)
    drain(to_chip, x_send)
    drain(to_chip, d_send)
    drain(to_chip, e_send)
    drain(to_core, pc_send)

    finish(stages - 1)
    taken = unpack(0, last, result[ep * cuts + last])
    out_ref[...] = (acc[...] + weight[:, 0:1] * taken).astype(jnp.bfloat16)
    drain(to_chip, px_send)


def fused(tokens, norm_gain, expert_ids, gate_weights, w_gate, w_up, w_down):
    tok_count, col_count = tokens.shape
    top_count = expert_ids.shape[1]
    n_ep = lax.axis_size("ep")
    n_tp = lax.axis_size("tp")
    cap = 3 * tok_count * top_count // (2 * n_ep)
    cuts = 2 if cap % 32 == 0 else 1
    stages, piece_rows = n_ep * cuts, cap // cuts
    width = norm_gain.shape[0]
    units = w_gate.shape[2]
    bf16 = jnp.bfloat16
    vmem = pl.BlockSpec(memory_space=pltpu.VMEM)
    anywhere = pl.BlockSpec(memory_space=pl.ANY)
    sems = pltpu.SemaphoreType.DMA
    return pl.pallas_call(
        functools.partial(layer_kernel, n_ep, cap, cuts),
        out_shape=jax.ShapeDtypeStruct((tok_count, col_count), bf16),
        in_specs=[anywhere] * 7,
        out_specs=vmem,
        scratch_shapes=[
            pltpu.VMEM((tok_count, col_count), bf16),
            pltpu.VMEM((top_count, tok_count), jnp.int32),
            pltpu.VMEM((top_count, tok_count), jnp.float32),
            pltpu.VMEM((1, width), jnp.float32),
            pltpu.VMEM((tok_count, col_count), jnp.float32),
            pltpu.VMEM((width, units), bf16),
            pltpu.VMEM((width, units), bf16),
            pltpu.VMEM((n_tp, units, col_count), bf16),
            pltpu.VMEM((stages, piece_rows, col_count), bf16),
            pltpu.VMEM((stages, n_tp, piece_rows, col_count), bf16),
            pltpu.VMEM((piece_rows, units), bf16),
            pltpu.VMEM((LAG + 1, piece_rows, col_count), jnp.float32),
            pltpu.VMEM((stages, 2, piece_rows, col_count), bf16),
            pltpu.VMEM((stages, 2, piece_rows, col_count), bf16),
        ]
        + [pltpu.VMEM((stages, piece_rows, col_count), bf16)] * 4
        + [sems((2 + n_tp,)), sems((4,))]
        + [sems, sems((stages,))] * 4
        + [sems, sems((stages, 2))]
        + [sems, sems((stages,))] * 2,
        compiler_params=pltpu.CompilerParams(
            collective_id=0, has_side_effects=True, vmem_limit_bytes=40 * 2**20
        ),
    )(
        *(
            pltpu.with_memory_space_constraint(operand, pltpu.HBM)
            for operand in (
                tokens,
                expert_ids.T,
                gate_weights.T,
                norm_gain.reshape(1, width),
                w_gate,
                w_up,
                w_down,
            )
        )
    )


def on_device(tokens, norm_gain, expert_ids, gate_weights, w_gate, w_up, w_down):
    tok_count = tokens.shape[0]
    top_count = expert_ids.shape[1]
    expert_count = lax.axis_size("ep")
    capacity = 3 * tok_count * top_count // (2 * expert_count)
    model_width = norm_gain.shape[0]
    flat_ids = expert_ids.reshape(-1)
    onehot = (flat_ids[:, None] == jnp.arange(expert_count, dtype=jnp.int32)[None, :]).astype(
        jnp.int32
    )
    earlier = jnp.cumsum(onehot, axis=0) - onehot
    slot_index = jnp.sum(earlier * onehot, axis=1)
    dest_index = flat_ids * capacity + slot_index
    owner_index = jnp.arange(tok_count * top_count, dtype=jnp.int32) // top_count
    slot_token = (
        jnp.full((expert_count * capacity,), tok_count, jnp.int32).at[dest_index].set(owner_index)
    )
    tok_values = tokens.astype(jnp.float32)
    square_sum = lax.psum(jnp.sum(tok_values * tok_values, axis=1, keepdims=True), "tp")
    col_count = tokens.shape[1]
    gain_part = lax.dynamic_slice_in_dim(norm_gain, lax.axis_index("tp") * col_count, col_count)
    normed = (tok_values * lax.rsqrt(square_sum / model_width + epsilon) * gain_part).astype(
        jnp.bfloat16
    )
    buffer = jnp.take(normed, slot_token, axis=0, mode="fill", fill_value=0).reshape(
        expert_count, capacity, -1
    )
    received = lax.all_to_all(buffer, "ep", split_axis=0, concat_axis=0, tiled=True)
    source_count, item_count, col_count = received.shape
    tok_rows = received.reshape(-1, col_count)
    col_piece = lax.all_gather(tok_rows, "tp", axis=1, tiled=True)
    gate_rows = w_gate[0]
    up_rows = w_up[0]
    gate_part = jnp.dot(col_piece, gate_rows, preferred_element_type=jnp.float32)
    up_part = jnp.dot(col_piece, up_rows, preferred_element_type=jnp.float32)
    hidden = (jax.nn.silu(gate_part) * up_part).astype(jnp.bfloat16)
    partial_value = jnp.dot(hidden, w_down[0], preferred_element_type=jnp.float32)
    partial_value = partial_value.reshape(source_count, item_count, -1)
    summed = lax.psum_scatter(
        partial_value.astype(jnp.bfloat16), "tp", scatter_dimension=2, tiled=True
    )
    came_back = lax.all_to_all(summed, "ep", split_axis=0, concat_axis=0, tiled=True)
    picked = came_back.reshape(expert_count * capacity, -1)[dest_index].astype(jnp.float32)
    weighted = picked * gate_weights.reshape(-1)[:, None]
    return jnp.sum(weighted.reshape(tok_count, top_count, -1), axis=1).astype(jnp.bfloat16)


def solution(mesh):
    return jax.shard_map(
        fused if mesh.shape["tp"] == 4 else on_device,
        mesh=mesh,
        in_specs=(
            P(("grp", "ep"), "tp"),
            P(),
            P(("grp", "ep"), None),
            P(("grp", "ep"), None),
            P("ep", None, "tp"),
            P("ep", None, "tp"),
            P("ep", "tp", None),
        ),
        out_specs=P(("grp", "ep"), "tp"),
        check_vma=False,
    )
```

```python
import functools

import jax
import jax.numpy as jnp
from jax import lax
from jax.experimental import pallas as pl
from jax.experimental.pallas import tpu as pltpu
from jax.sharding import PartitionSpec as P

epsilon = 1e-06
AHEAD = 2
LAG = 2
MESH = pl.DeviceIdType.MESH


def nearest_first(count):
    table = []
    for e in range(count):
        mirrored = 1 if 2 * e < count else -1
        table.append(sorted(range(count), key=lambda s: (abs(s - e), mirrored * s)))
    return table


def unit_order(n_ep, cuts):
    if (n_ep, cuts) == (4, 2):
        rows = [
            [(0, 1), (1, 0), (2, 1), (3, 0), (3, 1), (2, 0), (1, 1), (0, 0)],
            [(1, 1), (3, 0), (0, 1), (2, 0), (3, 1), (0, 0), (2, 1), (1, 0)],
            [(2, 1), (3, 1), (0, 0), (0, 1), (1, 0), (1, 1), (3, 0), (2, 0)],
            [(3, 1), (2, 0), (1, 1), (0, 0), (0, 1), (1, 0), (2, 1), (3, 0)],
        ]
    else:
        rows = [
            [(row[0], h) for h in range(cuts - 1)]
            + [(s, h) for s in row[1:] for h in range(cuts)]
            + [(row[0], cuts - 1)]
            for row in nearest_first(n_ep)
        ]
    return [[s * cuts + h for s, h in row] for row in rows]


def send_order(n_ep, cuts):
    if (n_ep, cuts) == (4, 2):
        rows = [
            [(2, 0), (1, 1), (1, 0), (3, 0), (2, 1), (3, 1)],
            [(0, 0), (3, 1), (2, 1), (3, 0), (2, 0), (0, 1)],
            [(0, 1), (3, 0), (1, 0), (1, 1), (0, 0), (3, 1)],
            [(1, 0), (2, 1), (2, 0), (0, 0), (1, 1), (0, 1)],
        ]
    else:
        rows = [
            [(s, h) for s in row[1:] for h in range(cuts)] for row in nearest_first(n_ep)
        ]
    return [[s * cuts + h for s, h in row] for row in rows]


def first_named(units, cuts):
    return list(dict.fromkeys(unit // cuts for unit in units))


def pick_row(table, row):
    picked = []
    for column in range(len(table[0])):
        value = jnp.int32(table[0][column])
        for r in range(1, len(table)):
            value = jnp.where(row == r, table[r][column], value)
        picked.append(value)
    return picked


def entry_of(entries, index):
    value = entries[0]
    for c in range(1, len(entries)):
        value = jnp.where(index == c, entries[c], value)
    return value


def layer_kernel(
    n_ep,
    cap,
    cuts,
    tok_hbm,
    ids_hbm,
    gate_hbm,
    gain_hbm,
    wg_ref,
    wu_ref,
    wd_ref,
    out_ref,
    tok_ref,
    ids_ref,
    gate_ref,
    gain_ref,
    acc,
    wg,
    wu,
    wd,
    packed,
    rows,
    hidden,
    own,
    to_core,
    from_core,
    to_chip,
    from_chip,
    result,
    back,
    w_sem,
    i_sem,
    z_send,
    z_recv,
    x_send,
    x_recv,
    d_send,
    d_recv,
    e_send,
    pc_send,
    pc_recv,
    px_send,
    px_recv,
    r_send,
    r_recv,
):
    tok_count, col_count = tok_ref.shape
    top_count = ids_ref.shape[0]
    n_tp = rows.shape[1]
    units = wg.shape[1]
    width = n_tp * col_count
    ep = lax.axis_index("ep")
    tp = lax.axis_index("tp")
    core = tp % 2
    sibling = tp + 1 - 2 * core
    across = (tp + 2) % n_tp
    side = tp // 2
    barrier = pltpu.get_barrier_semaphore()
    for step in range(1, n_ep):
        pl.semaphore_signal(
            barrier, inc=1, device_id={"ep": (ep + step) % n_ep}, device_id_type=MESH
        )
    for peer in (sibling, across):
        pl.semaphore_signal(barrier, inc=1, device_id={"tp": peer}, device_id_type=MESH)

    inputs = [
        pltpu.make_async_copy(source, target, i_sem.at[n])
        for n, (source, target) in enumerate(
            [
                (ids_hbm, ids_ref),
                (gate_hbm, gate_ref),
                (tok_hbm, tok_ref),
                (gain_hbm, gain_ref),
            ]
        )
    ]
    for copy in inputs:
        copy.start()

    order = [ep] + pick_row([first_named(row, cuts) for row in send_order(n_ep, cuts)], ep)
    turns = pick_row(unit_order(n_ep, cuts), ep)
    sends = pick_row(send_order(n_ep, cuts), ep)

    weights = [
        pltpu.make_async_copy(wg_ref.at[0], wg, w_sem.at[0]),
        pltpu.make_async_copy(wu_ref.at[0], wu, w_sem.at[1]),
    ]
    piece_of = [
        (1 - side) * 2 + 1 - core,
        side * 2 + 1 - core,
        (1 - side) * 2 + core,
        side * 2 + core,
    ]
    for j, piece in enumerate(piece_of):
        cols = pl.ds(pl.multiple_of(piece * col_count, col_count), col_count)
        weights.append(
            pltpu.make_async_copy(wd_ref.at[0, :, cols], wd.at[j], w_sem.at[2 + j])
        )
    inputs[0].wait()
    inputs[1].wait()
    columns = -(-n_ep // 16) * 16
    column = lax.broadcasted_iota(jnp.int32, (columns, tok_count), 0)
    column_expert = jnp.full((columns, tok_count), -1, jnp.int32)
    for i in range(n_ep):
        column_expert = jnp.where(column == i, order[i], column_expert)
    named = jnp.zeros((columns, tok_count), jnp.float32)
    weight_t = jnp.zeros((columns, tok_count), jnp.float32)
    for k in range(top_count):
        hit = ids_ref[k : k + 1, :] == column_expert
        named = named + jnp.where(hit, 1.0, 0.0)
        weight_t = weight_t + jnp.where(hit, gate_ref[k : k + 1, :], 0.0)
    before = jnp.where(
        lax.broadcasted_iota(jnp.int32, (tok_count, tok_count), 0)
        < lax.broadcasted_iota(jnp.int32, (tok_count, tok_count), 1),
        1.0,
        0.0,
    ).astype(jnp.bfloat16)
    place_t = jnp.dot(named.astype(jnp.bfloat16), before, preferred_element_type=jnp.float32)
    place_t = jnp.where(named > 0.0, place_t, -1.0)
    slot_rows = lax.broadcasted_iota(jnp.int32, (cap, tok_count), 0).astype(jnp.float32)

    def pack(i):
        pick = jnp.where(slot_rows == place_t[i : i + 1, :], 1.0, 0.0).astype(jnp.bfloat16)
        return jnp.dot(pick, tok_ref[...], preferred_element_type=jnp.float32).astype(
            jnp.bfloat16
        )

    def z_copy(here, there, h):
        return pltpu.make_async_remote_copy(
            src_ref=packed.at[there * cuts + h],
            dst_ref=rows.at[here * cuts + h, tp],
            send_sem=z_send,
            recv_sem=z_recv.at[here * cuts + h],
            device_id={"ep": there},
            device_id_type=MESH,
        )

    def x_copy(i):
        return pltpu.make_async_remote_copy(
            src_ref=rows.at[i, tp],
            dst_ref=rows.at[i, tp],
            send_sem=x_send,
            recv_sem=x_recv.at[i],
            device_id={"tp": across},
            device_id_type=MESH,
        )

    def d_copy(i):
        return pltpu.make_async_remote_copy(
            src_ref=rows.at[i, tp],
            dst_ref=rows.at[i, tp],
            send_sem=d_send,
            recv_sem=d_recv.at[i],
            device_id={"tp": sibling},
            device_id_type=MESH,
        )

    def e_copy(i):
        return pltpu.make_async_remote_copy(
            src_ref=rows.at[i, across],
            dst_ref=rows.at[i, across],
            send_sem=e_send,
            recv_sem=d_recv.at[i],
            device_id={"tp": sibling},
            device_id_type=MESH,
        )

    def pc_copy(i, j):
        return pltpu.make_async_remote_copy(
            src_ref=to_core.at[i, j],
            dst_ref=from_core.at[i, j],
            send_sem=pc_send,
            recv_sem=pc_recv.at[i, j],
            device_id={"tp": sibling},
            device_id_type=MESH,
        )

    def px_copy(i):
        return pltpu.make_async_remote_copy(
            src_ref=to_chip.at[i],
            dst_ref=from_chip.at[i],
            send_sem=px_send,
            recv_sem=px_recv.at[i],
            device_id={"tp": across},
            device_id_type=MESH,
        )

    def r_copy(here, there, h):
        return pltpu.make_async_remote_copy(
            src_ref=result.at[there * cuts + h],
            dst_ref=back.at[here * cuts + h],
            send_sem=r_send,
            recv_sem=r_recv.at[here * cuts + h],
            device_id={"ep": there},
            device_id_type=MESH,
        )

    piece_rows = cap // cuts
    stages = n_ep * cuts
    inputs[2].wait()
    for copy in weights[:2]:
        copy.start()
    values = pack(0)
    for h in range(cuts):
        rows[ep * cuts + h, tp] = values[h * piece_rows : (h + 1) * piece_rows]

    def unit_of(i):
        return turns[i] if isinstance(i, int) else entry_of(turns, i)

    def spread(s):
        x_copy(s).start()
        d_copy(s).start()

    def forward(i):
        s = unit_of(i)

        @pl.when(s // cuts != ep)
        def _():
            z_copy(s // cuts, s // cuts, s % cuts).wait_recv()
            spread(s)

    pl.semaphore_wait(barrier, n_ep + 1)
    first = turns[0] % cuts
    for step in range(cuts):
        spread(ep * cuts + (first + step) % cuts)
    for i in range(1, n_ep):
        values = pack(i)
        for h in range(cuts):
            packed[order[i] * cuts + h] = values[h * piece_rows : (h + 1) * piece_rows]
        for unit in sends[i - 1 :] if i + 1 == n_ep else sends[i - 1 : i]:
            z_copy(ep, unit // cuts, unit % cuts).start()
    inputs[3].wait()
    for copy in weights[:2]:
        copy.wait()
    for copy in weights[2:]:
        copy.start()

    def scale(i, carry):
        block = pl.ds(pl.multiple_of(i * 128, 128), 128)
        gain = jnp.broadcast_to(gain_ref[:, block], (128, 128)).T
        for matrix in (wg, wu):
            for c in range(units // 128):
                cols = slice(c * 128, (c + 1) * 128)
                matrix[block, cols] = (matrix[block, cols].astype(jnp.float32) * gain).astype(
                    jnp.bfloat16
                )
        return carry

    lax.fori_loop(0, width // 128, scale, 0, unroll=2)

    def finish(i):
        s = unit_of(i)
        pc_copy(s, 1).wait_recv()
        total = own[i % (LAG + 1)] + from_core[s, 1].astype(jnp.float32)
        px_copy(s).wait_recv()
        total = total + from_chip[s].astype(jnp.float32)
        result[s] = total.astype(jnp.bfloat16)

        @pl.when(s // cuts != ep)
        def _():
            r_copy(ep, s // cuts, s % cuts).start()

    for i in range(1, AHEAD):
        forward(i)
    x_copy(unit_of(0)).wait_recv()
    e_copy(unit_of(0)).start()
    for copy in weights[2:]:
        copy.wait()

    def stage(i, carry):
        s = unit_of(i)
        pair = rows.at[s, pl.ds(0, 2)]
        pltpu.make_async_remote_copy(
            src_ref=pair,
            dst_ref=pair,
            send_sem=d_send,
            recv_sem=d_recv.at[s],
            device_id={"tp": sibling},
            device_id_type=MESH,
        ).wait_recv()
        square_sum = jnp.zeros((piece_rows, 1), jnp.float32)
        for k in range(n_tp):
            part = rows[s, k].astype(jnp.float32)
            square_sum = square_sum + jnp.sum(part * part, axis=1, keepdims=True)
        factor = lax.rsqrt(square_sum / width + epsilon)
        for c in range(units // 256):
            cols = slice(c * 256, (c + 1) * 256)
            gate_part = jnp.zeros((piece_rows, 256), jnp.float32)
            up_part = jnp.zeros((piece_rows, 256), jnp.float32)
            for k in range(n_tp):
                depth = slice(k * col_count, (k + 1) * col_count)
                part = rows[s, k]
                gate_part = gate_part + jnp.dot(
                    part, wg[depth, cols], preferred_element_type=jnp.float32
                )
                up_part = up_part + jnp.dot(
                    part, wu[depth, cols], preferred_element_type=jnp.float32
                )
            gate_part = gate_part * factor
            up_part = up_part * factor
            hidden[:, cols] = (gate_part / (1.0 + jnp.exp(-gate_part)) * up_part).astype(
                jnp.bfloat16
            )

        @pl.when(i >= LAG)
        def _():
            finish(i - LAG)

        @pl.when(i + AHEAD < stages)
        def _():
            forward(i + AHEAD)

        to_core[s, 0] = jnp.dot(
            hidden[...], wd[0], preferred_element_type=jnp.float32
        ).astype(jnp.bfloat16)
        pc_copy(s, 0).start()
        to_core[s, 1] = jnp.dot(
            hidden[...], wd[1], preferred_element_type=jnp.float32
        ).astype(jnp.bfloat16)
        part = jnp.dot(hidden[...], wd[2], preferred_element_type=jnp.float32)
        own[i % (LAG + 1)] = jnp.dot(hidden[...], wd[3], preferred_element_type=jnp.float32)
        pc_copy(s, 1).start()

        @pl.when(i + 2 < stages)
        def _():
            after = unit_of(i + 1)
            x_copy(after).wait_recv()
            e_copy(after).start()

        @pl.when(i == 1)
        def _():
            x_copy(unit_of(stages - 1)).wait_recv()
            e_copy(unit_of(stages - 1)).start()

        pc_copy(s, 0).wait_recv()
        to_chip[s] = (part + from_core[s, 0].astype(jnp.float32)).astype(jnp.bfloat16)
        px_copy(s).start()

        return carry

    lax.fori_loop(0, stages, stage, 0)
    for i in range(stages - LAG, stages - 1):
        finish(i)

    slot_lanes = lax.broadcasted_iota(jnp.int32, (tok_count, piece_rows), 1).astype(
        jnp.float32
    )

    place = place_t.T
    weight = weight_t.T

    def unpack(i, h, values):
        start = jnp.asarray(h * piece_rows, jnp.int32).astype(jnp.float32)
        pick = jnp.where(slot_lanes + start == place[:, i : i + 1], 1.0, 0.0)
        return jnp.dot(pick.astype(jnp.bfloat16), values, preferred_element_type=jnp.float32)

    mixed = jnp.zeros((tok_count, col_count), jnp.float32)
    for i in range(1, n_ep):
        taken = jnp.zeros((tok_count, col_count), jnp.float32)
        for h in range(cuts):
            r_copy(order[i], order[i], h).wait_recv()
            taken = taken + unpack(i, h, back[order[i] * cuts + h])
        mixed = mixed + weight[:, i : i + 1] * taken
    last = turns[stages - 1] % cuts
    for step in range(1, cuts):
        h = (last + step) % cuts
        mixed = mixed + weight[:, 0:1] * unpack(0, h, result[ep * cuts + h])
    acc[...] = mixed

    def drain(pieces, sem):
        pltpu.make_async_remote_copy(
            src_ref=pieces,
            dst_ref=pieces,
            send_sem=sem,
            recv_sem=px_recv.at[0],
            device_id={"tp": across},
            device_id_type=MESH,
        ).wait_send()

    others = stages - cuts
    drain(packed.at[pl.ds(0, others)], z_send)
    drain(result.at[pl.ds(0, others)], r_send)
    drain(to_chip, x_send)
    drain(to_chip, d_send)
    drain(to_chip, e_send)
    drain(to_core, pc_send)

    finish(stages - 1)
    taken = unpack(0, last, result[ep * cuts + last])
    out_ref[...] = (acc[...] + weight[:, 0:1] * taken).astype(jnp.bfloat16)
    drain(to_chip, px_send)


def fused(tokens, norm_gain, expert_ids, gate_weights, w_gate, w_up, w_down):
    tok_count, col_count = tokens.shape
    top_count = expert_ids.shape[1]
    n_ep = lax.axis_size("ep")
    n_tp = lax.axis_size("tp")
    cap = 3 * tok_count * top_count // (2 * n_ep)
    cuts = 2 if cap % 32 == 0 else 1
    stages, piece_rows = n_ep * cuts, cap // cuts
    width = norm_gain.shape[0]
    units = w_gate.shape[2]
    bf16 = jnp.bfloat16
    vmem = pl.BlockSpec(memory_space=pltpu.VMEM)
    anywhere = pl.BlockSpec(memory_space=pl.ANY)
    sems = pltpu.SemaphoreType.DMA
    return pl.pallas_call(
        functools.partial(layer_kernel, n_ep, cap, cuts),
        out_shape=jax.ShapeDtypeStruct((tok_count, col_count), bf16),
        in_specs=[anywhere] * 7,
        out_specs=vmem,
        scratch_shapes=[
            pltpu.VMEM((tok_count, col_count), bf16),
            pltpu.VMEM((top_count, tok_count), jnp.int32),
            pltpu.VMEM((top_count, tok_count), jnp.float32),
            pltpu.VMEM((1, width), jnp.float32),
            pltpu.VMEM((tok_count, col_count), jnp.float32),
            pltpu.VMEM((width, units), bf16),
            pltpu.VMEM((width, units), bf16),
            pltpu.VMEM((n_tp, units, col_count), bf16),
            pltpu.VMEM((stages, piece_rows, col_count), bf16),
            pltpu.VMEM((stages, n_tp, piece_rows, col_count), bf16),
            pltpu.VMEM((piece_rows, units), bf16),
            pltpu.VMEM((LAG + 1, piece_rows, col_count), jnp.float32),
            pltpu.VMEM((stages, 2, piece_rows, col_count), bf16),
            pltpu.VMEM((stages, 2, piece_rows, col_count), bf16),
        ]
        + [pltpu.VMEM((stages, piece_rows, col_count), bf16)] * 4
        + [sems((2 + n_tp,)), sems((4,))]
        + [sems, sems((stages,))] * 3
        + [sems]
        + [sems, sems((stages, 2))]
        + [sems, sems((stages,))] * 2,
        compiler_params=pltpu.CompilerParams(
            collective_id=0, has_side_effects=True, vmem_limit_bytes=40 * 2**20
        ),
    )(
        *(
            pltpu.with_memory_space_constraint(operand, pltpu.HBM)
            for operand in (
                tokens,
                expert_ids.T,
                gate_weights.T,
                norm_gain.reshape(1, width),
                w_gate,
                w_up,
                w_down,
            )
        )
    )


def on_device(tokens, norm_gain, expert_ids, gate_weights, w_gate, w_up, w_down):
    tok_count = tokens.shape[0]
    top_count = expert_ids.shape[1]
    expert_count = lax.axis_size("ep")
    capacity = 3 * tok_count * top_count // (2 * expert_count)
    model_width = norm_gain.shape[0]
    flat_ids = expert_ids.reshape(-1)
    onehot = (flat_ids[:, None] == jnp.arange(expert_count, dtype=jnp.int32)[None, :]).astype(
        jnp.int32
    )
    earlier = jnp.cumsum(onehot, axis=0) - onehot
    slot_index = jnp.sum(earlier * onehot, axis=1)
    dest_index = flat_ids * capacity + slot_index
    owner_index = jnp.arange(tok_count * top_count, dtype=jnp.int32) // top_count
    slot_token = (
        jnp.full((expert_count * capacity,), tok_count, jnp.int32).at[dest_index].set(owner_index)
    )
    tok_values = tokens.astype(jnp.float32)
    square_sum = lax.psum(jnp.sum(tok_values * tok_values, axis=1, keepdims=True), "tp")
    col_count = tokens.shape[1]
    gain_part = lax.dynamic_slice_in_dim(norm_gain, lax.axis_index("tp") * col_count, col_count)
    normed = (tok_values * lax.rsqrt(square_sum / model_width + epsilon) * gain_part).astype(
        jnp.bfloat16
    )
    buffer = jnp.take(normed, slot_token, axis=0, mode="fill", fill_value=0).reshape(
        expert_count, capacity, -1
    )
    received = lax.all_to_all(buffer, "ep", split_axis=0, concat_axis=0, tiled=True)
    source_count, item_count, col_count = received.shape
    tok_rows = received.reshape(-1, col_count)
    col_piece = lax.all_gather(tok_rows, "tp", axis=1, tiled=True)
    gate_rows = w_gate[0]
    up_rows = w_up[0]
    gate_part = jnp.dot(col_piece, gate_rows, preferred_element_type=jnp.float32)
    up_part = jnp.dot(col_piece, up_rows, preferred_element_type=jnp.float32)
    hidden = (jax.nn.silu(gate_part) * up_part).astype(jnp.bfloat16)
    partial_value = jnp.dot(hidden, w_down[0], preferred_element_type=jnp.float32)
    partial_value = partial_value.reshape(source_count, item_count, -1)
    summed = lax.psum_scatter(
        partial_value.astype(jnp.bfloat16), "tp", scatter_dimension=2, tiled=True
    )
    came_back = lax.all_to_all(summed, "ep", split_axis=0, concat_axis=0, tiled=True)
    picked = came_back.reshape(expert_count * capacity, -1)[dest_index].astype(jnp.float32)
    weighted = picked * gate_weights.reshape(-1)[:, None]
    return jnp.sum(weighted.reshape(tok_count, top_count, -1), axis=1).astype(jnp.bfloat16)


def solution(mesh):
    return jax.shard_map(
        fused if mesh.shape["tp"] == 4 else on_device,
        mesh=mesh,
        in_specs=(
            P(("grp", "ep"), "tp"),
            P(),
            P(("grp", "ep"), None),
            P(("grp", "ep"), None),
            P("ep", None, "tp"),
            P("ep", None, "tp"),
            P("ep", "tp", None),
        ),
        out_specs=P(("grp", "ep"), "tp"),
        check_vma=False,
    )
```
